32 devices in a mesh: sp: 8 (over z, y), tp: 4 (over x, core).
Axes of the slice: x: 2, y: 2, z: 4, core: 2. Of those that a mesh axis runs over, the one named last changes fastest.
Arguments:
- queries: bfloat16 [4096, 1024], P('sp', 'tp'), may hold values from -60 to 60
- keys: bfloat16 [4096, 1024], P('sp', 'tp'), may hold values from -6 to 6
- values: bfloat16 [4096, 1024], P('sp', 'tp'), may hold values from -6 to 6
- lambdas: float32 [8], P('tp'), may hold values from 0.3 to 0.8
- head_gain: float32 [128], replicated, may hold values from 0.1 to 1.9
- w_out: bfloat16 [1024, 2048], replicated, may hold values from -0.1875 to 0.1875
- residual_in: bfloat16 [4096, 2048], P(('sp', 'tp')), may hold values from -6 to 6
- norm_gain: float32 [2048], replicated, may hold values from 0.1 to 1.9
- route_ids: int32 [4096, 2], P(('sp', 'tp')), may hold values from 0 to 7, as said below
- route_weight: float32 [4096, 2], P(('sp', 'tp')), may hold values from 0.2 to 1
- w_gate: bfloat16 [8, 2048, 1024], P('sp', None, 'tp'), may hold values from -0.125 to 0.125
- w_up: bfloat16 [8, 2048, 1024], P('sp', None, 'tp'), may hold values from -0.125 to 0.125
- w_down: bfloat16 [8, 2048, 1024], P('sp', None, 'tp'), may hold values from -0.1875 to 0.1875
Outputs:
- layer_out: bfloat16 [4096, 2048], P(('sp', 'tp'))
The draws below stay inside these ranges and needn't reach their ends.
Inputs may be any that keep to these rules, and one draw needn't show every extreme that they name: `route_ids`: each row names two different experts of one group (the same expert // 8). Among the 128 rows of one device (aligned blocks), no expert is named more than 64 times, and in every draw one expert is named exactly 64 times in the rows of every device.
All inputs are finite; a program needn't handle non-finite values.
Results may differ from the reference program's by a relative error of at most 0.015.
Values may be sent and summed in bfloat16 or wider, within the bound.
A program may use at most 128 MiB of HBM per device.

```python
import jax
import jax.numpy as jnp
from jax import lax

D = 2048
HEADS = 8
HEAD_DIM = 64
FF = 1024
GROUP_SIZE = 8
SEQ_LEN = 4096
SEQUENCES = 1
TOKENS = 4096
DEV_ROWS = 128
EXPERTS = 8
GROUPS = 1
CAPACITY = 64


def base_field(key, salt_value):
    array_shape = (TOKENS, HEADS * 2 * HEAD_DIM)
    subkey = jax.random.fold_in(key, salt_value)
    return jnp.clip(1.3 * jax.random.normal(subkey, array_shape, jnp.float32), -5.5, 5.5)


def draw_keys(key, part):
    base_values = base_field(key, 11)
    return base_values.astype(jnp.bfloat16)


def draw_queries(key, part):
    base_values = base_field(key, 12)
    return base_values.astype(jnp.bfloat16)


def draw_route_ids(key, part):
    block_count = TOKENS // DEV_ROWS
    pair_count = EXPERTS * CAPACITY // 2
    favored = jax.random.randint(jax.random.fold_in(key, 31), (), 0, EXPERTS)
    round_offsets = (jnp.arange(GROUPS * CAPACITY, dtype=jnp.int32) // CAPACITY)[:, None] * GROUP_SIZE

    def one_block(block_key):
        round_keys = jax.random.split(jax.random.fold_in(block_key, 1), GROUPS * CAPACITY)
        rounds = jax.vmap(lambda round_key: jax.random.permutation(round_key, GROUP_SIZE))(round_keys)
        pair_table = (rounds.astype(jnp.int32) + round_offsets).reshape(pair_count, 2)
        holds_favored = jnp.any(pair_table == favored, axis=1).astype(jnp.int32)
        jitter_values = jax.random.randint(jax.random.fold_in(block_key, 2), (pair_count,), 0, 1 << 18)
        priority = (jitter_values + holds_favored * (1 << 18)) * pair_count + jnp.arange(pair_count, dtype=jnp.int32)
        unused, picked = lax.top_k(priority, DEV_ROWS)
        shuffle = jax.random.permutation(jax.random.fold_in(block_key, 3), DEV_ROWS)
        return pair_table[picked][shuffle]
    block_keys = jax.vmap(lambda block_index: jax.random.fold_in(jax.random.fold_in(key, 32), block_index))(jnp.arange(block_count))
    return jax.vmap(one_block)(block_keys).reshape(TOKENS, 2).astype(jnp.int32)


def steps_of(own_key, shape, shards, low, largest):
    level = 1.0
    for position, parts in shards:
        steps = jax.random.uniform(jax.random.fold_in(jax.random.fold_in(own_key, 6), position), (parts,), jnp.float32, low / len(shards), largest / len(shards))
        level = level * jnp.repeat(jnp.exp(steps), shape[position] // parts).reshape((-1,) + (1,) * (len(shape) - 1 - position))
    return level


def scatter_about(stream_key, shape, deviation, reach, shards=(), held_as=jnp.bfloat16):
    drawn = deviation * jax.random.normal(stream_key, shape, jnp.float32)
    if shards:
        drawn = drawn * steps_of(stream_key, shape, shards, -0.22, 0.18)
    return jnp.clip(drawn, -reach, reach).astype(held_as)


def setup_inputs(seed: int = 0) -> dict:
    splits = jax.random.split(jax.random.key(seed), 14)
    queries = draw_queries(jax.random.fold_in(splits[13], 71), 0)
    keys = draw_keys(jax.random.fold_in(splits[13], 71), 0)
    values = scatter_about(splits[2], (TOKENS, HEADS * 2 * HEAD_DIM), 1.0, 6.0, ((0, 8), (1, 4)))
    lambdas = jnp.clip(0.3 + 0.5 * jax.random.uniform(splits[3], (HEADS,), jnp.float32) ** steps_of(splits[3], (HEADS,), ((0, 4),), -0.2, 0.2), 0.3, 0.8)
    head_gain = jnp.clip(1.0 + 0.18 * jax.random.normal(splits[4], (2 * HEAD_DIM,), jnp.float32), 0.1, 1.9)
    w_out = scatter_about(splits[5], (HEADS * 2 * HEAD_DIM, D), (HEADS * 2 * HEAD_DIM) ** -0.5, 0.1875)
    residual_in = scatter_about(splits[6], (TOKENS, D), 1.0, 6.0, ((0, 32),))
    norm_gain = jnp.clip(1.0 + 0.18 * jax.random.normal(splits[7], (D,), jnp.float32), 0.1, 1.9)
    route_ids = draw_route_ids(jax.random.fold_in(splits[13], 71), 0)
    route_weight = jnp.clip(0.2 + 0.8 * jax.random.uniform(splits[9], (TOKENS, 2), jnp.float32) ** steps_of(splits[9], (TOKENS, 2), ((0, 32),), -0.2, 0.2), 0.2, 1.0)
    w_gate = scatter_about(splits[10], (EXPERTS, D, FF), D ** -0.5, 0.125, ((0, 8), (2, 4)))
    w_up = scatter_about(splits[11], (EXPERTS, D, FF), D ** -0.5, 0.125, ((0, 8), (2, 4)))
    w_down = scatter_about(splits[12], (EXPERTS, D, FF), FF ** -0.5, 0.1875, ((0, 8), (2, 4)))
    return {"queries": queries, "keys": keys, "values": values, "lambdas": lambdas, "head_gain": head_gain, "w_out": w_out, "residual_in": residual_in, "norm_gain": norm_gain, "route_ids": route_ids, "route_weight": route_weight, "w_gate": w_gate, "w_up": w_up, "w_down": w_down}


EPSILON = 1e-06
OUT_SCALE = 0.8

def slot_numbers(flat_ids):
    count_ids = flat_ids.shape[0]
    positions = lax.broadcasted_iota(jnp.int32, (count_ids, count_ids), 0)
    earlier = lax.broadcasted_iota(jnp.int32, (count_ids, count_ids), 1) < positions
    matches = (flat_ids[:, None] == flat_ids[None, :]) & earlier
    return lax.optimization_barrier(jnp.sum(matches.astype(jnp.int32), axis=1))

def attend_block(query_block, key_view, value_view, lambdas, head_gain):
    scores = jnp.einsum('qhmd,khmd->hmqk', query_block.astype(jnp.float32), key_view) * HEAD_DIM ** (-0.5)
    peak_score = lax.optimization_barrier(jnp.max(scores, axis=-1, keepdims=True))
    weights = jnp.exp(scores - peak_score)
    totals = lax.optimization_barrier(jnp.sum(weights, axis=-1))
    rounded = lax.optimization_barrier(weights.astype(jnp.bfloat16)).astype(jnp.float32)
    numerators = jnp.einsum('hmqk,khv->hmqv', rounded, value_view)
    heads_out = numerators / totals[..., None]
    combined = heads_out[:, 0] - lambdas[:, None, None] * heads_out[:, 1]
    mean_square = lax.optimization_barrier(jnp.mean(combined * combined, axis=-1, keepdims=True))
    normalized = combined * lax.rsqrt(mean_square + EPSILON) * head_gain * OUT_SCALE
    return jnp.transpose(normalized, (1, 0, 2)).reshape(query_block.shape[0], -1).astype(jnp.bfloat16)

def attend_sequence(operands, lambdas, head_gain):
    seq_queries, seq_keys, seq_values = operands
    query_view = seq_queries.reshape(SEQ_LEN // 128, 128, HEADS, 2, HEAD_DIM)
    key_view = seq_keys.reshape(SEQ_LEN, HEADS, 2, HEAD_DIM).astype(jnp.float32)
    value_view = seq_values.reshape(SEQ_LEN, HEADS, 2 * HEAD_DIM).astype(jnp.float32)
    return lax.map(lambda query_block: attend_block(query_block, key_view, value_view, lambdas, head_gain), query_view)

def run_expert(operands):
    rows_in, gate_weight, up_weight, down_weight = operands
    gate_proj = jnp.dot(rows_in, gate_weight, preferred_element_type=jnp.float32)
    up_proj = jnp.dot(rows_in, up_weight, preferred_element_type=jnp.float32)
    hidden_units = (jax.nn.silu(gate_proj) * up_proj).astype(jnp.bfloat16)
    return jnp.dot(hidden_units, down_weight.T, preferred_element_type=jnp.float32).astype(jnp.bfloat16)

def reference(queries, keys, values, lambdas, head_gain, w_out, residual_in, norm_gain, route_ids, route_weight, w_gate, w_up, w_down):
    width = HEADS * 2 * HEAD_DIM
    seq_shape = (SEQUENCES, SEQ_LEN, width)
    attended = lax.map(lambda operands: attend_sequence(operands, lambdas, head_gain), (queries.reshape(seq_shape), keys.reshape(seq_shape), values.reshape(seq_shape)))
    attended = attended.reshape(TOKENS, width)
    mixed_out = jnp.dot(attended, w_out, preferred_element_type=jnp.float32).astype(jnp.bfloat16)
    carried = (residual_in.astype(jnp.float32) + mixed_out.astype(jnp.float32)).astype(jnp.bfloat16)
    carried_wide = carried.astype(jnp.float32)
    normed = (carried_wide * lax.rsqrt(lax.optimization_barrier(jnp.mean(carried_wide * carried_wide, axis=-1, keepdims=True)) + EPSILON) * norm_gain).astype(jnp.bfloat16)
    blocks = TOKENS // DEV_ROWS
    flat_ids = route_ids.reshape(blocks, 2 * DEV_ROWS)
    slot_index = jax.vmap(slot_numbers)(flat_ids)
    targets = (flat_ids * CAPACITY + slot_index).astype(jnp.int32)
    sources = jnp.repeat(normed.reshape(blocks, DEV_ROWS, D), 2, axis=1)
    block_index = jnp.broadcast_to(jnp.arange(blocks, dtype=jnp.int32)[:, None], targets.shape)
    buffers = jnp.zeros((blocks, EXPERTS * CAPACITY, D), jnp.bfloat16).at[block_index, targets].set(sources)
    per_expert = jnp.moveaxis(buffers.reshape(blocks, EXPERTS, CAPACITY, D), 1, 0).reshape(EXPERTS, blocks * CAPACITY, D)
    outputs = lax.map(run_expert, (per_expert, w_gate, w_up, w_down))
    returned = jnp.moveaxis(outputs.reshape(EXPERTS, blocks, CAPACITY, D), 0, 1).reshape(blocks, EXPERTS * CAPACITY, D)
    picked = returned[block_index, targets].astype(jnp.float32).reshape(TOKENS, 2, D)
    layer_out = carried.astype(jnp.float32) + lax.optimization_barrier(jnp.sum(route_weight[..., None] * picked, axis=1))
    return layer_out.astype(jnp.bfloat16)
```

```python
import functools
import math

import jax
import jax.numpy as jnp
from jax import lax
from jax.experimental import pallas as pl
from jax.experimental.pallas import tpu as pltpu
from jax.sharding import PartitionSpec as P

EPSILON = 1e-06
OUT_SCALE = 0.8
FLOOR_SCORE = -1e30


def swapped(value, axis, distance):
    mask = 2**distance
    pairs = [(source, source ^ mask) for source in range(lax.axis_size(axis))]
    return lax.ppermute(value, axis, pairs)


def slot_numbers(flat_ids):
    count_ids = flat_ids.shape[0]
    positions = lax.broadcasted_iota(jnp.int32, (count_ids, count_ids), 0)
    earlier = lax.broadcasted_iota(jnp.int32, (count_ids, count_ids), 1) < positions
    matches = (flat_ids[:, None] == flat_ids[None, :]) & earlier
    return jnp.sum(matches.astype(jnp.int32), axis=1)


def send_back(results):
    return lax.all_to_all(results, "sp", split_axis=0, concat_axis=0, tiled=True)

MESH = pl.DeviceIdType.MESH
VMEM_BYTES = 60 * 1024 * 1024


def ring_neighbours(group):
    me = lax.axis_index("sp")
    spot = lax.rem(me, group)
    base = me - spot
    even = lax.rem(spot, 2) == 0
    up = jnp.where(even, jnp.where(spot == group - 2, group - 1, spot + 2), jnp.where(spot == 1, 0, spot - 2))
    down = jnp.where(even, jnp.where(spot == 0, 1, spot - 2), jnp.where(spot == group - 1, group - 2, spot + 2))
    return base + up, base + down


def attention_kernel(
    group,
    tp,
    q_ref,
    k_ref,
    v_ref,
    lam_ref,
    gain_ref,
    w_out_ref,
    residual_ref,
    norm_gain_ref,
    gate_ref,
    up_ref,
    carried_ref,
    normed_ref,
    far_gate_ref,
    far_up_ref,
    k_slots,
    v_slots,
    q_masked,
    peaks,
    totals,
    numerators,
    made,
    came,
    w_out_here,
    send_sems,
    recv_sems,
    row_send,
    row_recv,
    load_sems,
    far_send,
    far_recv,
):
    rows = q_ref.shape[0]
    heads = lam_ref.shape[0]
    value_dim = v_ref.shape[1] // heads
    head_dim = value_dim // 2
    exponent_scale = head_dim ** (-0.5) * math.log2(math.e)
    right, left = ring_neighbours(group)
    me_tp = lax.axis_index("tp")

    barrier = pltpu.get_barrier_semaphore()
    for neighbour in (right, left):
        pl.semaphore_signal(barrier, inc=1, device_id={"sp": neighbour}, device_id_type=MESH)
    for step in range(1, tp):
        pl.semaphore_signal(
            barrier, inc=1, device_id={"tp": lax.rem(me_tp + step, tp)}, device_id_type=MESH
        )
    pl.semaphore_wait(barrier, 2 + tp - 1)

    def send(source, slots, which, slot, target):
        return pltpu.make_async_remote_copy(
            src_ref=source,
            dst_ref=slots.at[slot],
            send_sem=send_sems.at[which, slot],
            recv_sem=recv_sems.at[which, slot],
            device_id={"sp": target},
            device_id_type=MESH,
        )

    last = group - 1
    if group > 2:
        for slot, target in ((1, right), (2, left)):
            send(k_ref, k_slots, 0, slot, target).start()
            send(v_ref, v_slots, 1, slot, target).start()
    elif group == 2:
        send(k_ref, k_slots, 0, 1, right).start()
        send(v_ref, v_slots, 1, 1, left).start()
    own_loads = (
        pltpu.make_async_copy(k_ref, k_slots.at[0], load_sems.at[0]),
        pltpu.make_async_copy(v_ref, v_slots.at[0], load_sems.at[1]),
    )
    for load in own_loads:
        load.start()
    load_w_out = pltpu.make_async_copy(w_out_ref, w_out_here, load_sems.at[2])
    load_w_out.start()

    far_copies = [
        pltpu.make_async_remote_copy(
            src_ref=source,
            dst_ref=landing,
            send_sem=far_send.at[index],
            recv_sem=far_recv.at[index],
            device_id={"tp": lax.rem(me_tp + tp // 2, tp)},
            device_id_type=MESH,
        )
        for index, (source, landing) in enumerate(((gate_ref, far_gate_ref), (up_ref, far_up_ref)))
    ]
    for copy in far_copies:
        copy.start()

    lane = lax.broadcasted_iota(jnp.int32, (rows, value_dim), 1)
    for head in range(heads):
        both = q_ref[:, head * value_dim : (head + 1) * value_dim]
        q_masked[2 * head] = jnp.where(lane < head_dim, both, jnp.zeros_like(both))
        q_masked[2 * head + 1] = jnp.where(lane >= head_dim, both, jnp.zeros_like(both))
    peaks[...] = jnp.full(peaks.shape, FLOOR_SCORE, jnp.float32)
    totals[...] = jnp.zeros(totals.shape, jnp.float32)
    numerators[...] = jnp.zeros(numerators.shape, jnp.float32)
    for load in own_loads:
        load.wait()

    chunk = min(rows, 256)

    def absorb(slot, count):
        keys_here = count * k_slots.shape[1]
        for head in range(heads):
            columns = slice(head * value_dim, (head + 1) * value_dim)
            key_block = k_slots[pl.ds(slot, count), :, columns].reshape(keys_here, value_dim)
            value_block = v_slots[pl.ds(slot, count), :, columns].reshape(keys_here, value_dim)
            with_ones = jnp.concatenate(
                [value_block, jnp.ones((keys_here, 128), jnp.bfloat16)], axis=1
            )
            for part in (2 * head, 2 * head + 1):
                for begin in range(0, rows, chunk):
                    here = slice(begin, begin + chunk)
                    scores = lax.dot_general(
                        q_masked[part, here],
                        key_block,
                        (((1,), (1,)), ((), ())),
                        preferred_element_type=jnp.float32,
                    )
                    old_peak = peaks[part, here][:, :1]
                    new_peak = jnp.maximum(old_peak, jnp.max(scores, axis=1, keepdims=True))
                    weights = jnp.exp2((scores - new_peak) * exponent_scale)
                    shrink = jnp.exp2((old_peak - new_peak) * exponent_scale)
                    product = jnp.dot(
                        weights.astype(jnp.bfloat16), with_ones, preferred_element_type=jnp.float32
                    )
                    numerators[part, here] = (
                        numerators[part, here] * shrink + product[:, :value_dim]
                    )
                    totals[part, here] = totals[part, here] * shrink + product[:, value_dim:]
                    peaks[part, here] = jnp.broadcast_to(new_peak, (chunk, 128))

    def one_pair(pair, unused):
        slot = 2 * pair + 1

        def pass_on(which, slots, at, target):
            send(slots.at[at], slots, which, at, target).wait_recv()

            @pl.when(at + 2 <= last - 1)
            def _():
                send(slots.at[at], slots, which, at + 2, target).start()

        for which, slots in ((0, k_slots), (1, v_slots)):
            pass_on(which, slots, slot, right)
            if which == 0:

                @pl.when(slot == last - 2)
                def _():
                    send(slots.at[slot], slots, which, last, right).start()

            pass_on(which, slots, slot + 1, left)
            if which == 1:

                @pl.when(slot == last - 2)
                def _():
                    send(slots.at[slot + 1], slots, which, last, left).start()

        absorb(slot, 2)
        return unused

    absorb(0, 1)
    lax.fori_loop(0, (group - 2) // 2, one_pair, 0)
    if last:
        send(k_slots.at[last], k_slots, 0, last, right).wait_recv()
        send(v_slots.at[last], v_slots, 1, last, left).wait_recv()
        absorb(last, 1)

    gain = gain_ref[...] * OUT_SCALE
    for head in range(heads):
        first = numerators[2 * head] / totals[2 * head][:, :1]
        second = numerators[2 * head + 1] / totals[2 * head + 1][:, :1]
        combined = first - lam_ref[head] * second
        mean_square = jnp.mean(combined * combined, axis=1, keepdims=True)
        made[:, head * value_dim : (head + 1) * value_dim] = (
            combined * lax.rsqrt(mean_square + EPSILON) * gain
        ).astype(jnp.bfloat16)

    dev_rows = residual_ref.shape[0]

    def row_copy(step, owner, target):
        return pltpu.make_async_remote_copy(
            src_ref=made.at[pl.ds(pl.multiple_of(target * dev_rows, dev_rows), dev_rows)],
            dst_ref=came.at[owner],
            send_sem=row_send.at[step],
            recv_sem=row_recv.at[step],
            device_id={"tp": target},
            device_id_type=MESH,
        )

    sends = [row_copy(step, me_tp, lax.rem(me_tp + step, tp)) for step in range(1, tp)]
    for copy in sends:
        copy.start()
    came[me_tp] = made[pl.ds(pl.multiple_of(me_tp * dev_rows, dev_rows), dev_rows)]
    load_w_out.wait()
    for step in range(1, tp):
        row_copy(
            step, lax.rem(me_tp + tp - step, tp), lax.rem(me_tp + step, tp)
        ).wait_recv()
    attended = jnp.concatenate([came[peer] for peer in range(tp)], axis=1)
    mixed = jnp.dot(attended, w_out_here[...], preferred_element_type=jnp.float32).astype(
        jnp.bfloat16
    )
    carried = (residual_ref[...].astype(jnp.float32) + mixed.astype(jnp.float32)).astype(
        jnp.bfloat16
    )
    carried_ref[...] = carried
    wide = carried.astype(jnp.float32)
    spread = jnp.mean(wide * wide, axis=1, keepdims=True)
    normed_ref[...] = (wide * lax.rsqrt(spread + EPSILON) * norm_gain_ref[...]).astype(
        jnp.bfloat16
    )
    for copy in sends:
        copy.wait_send()
    for slot in range(1, group):
        send(k_ref, k_slots, 0, slot, right).wait_send()
        send(v_ref, v_slots, 1, slot, right).wait_send()
    for copy in far_copies:
        copy.wait()


def attend(queries, keys, values, lambdas, head_gain, w_out, residual_in, norm_gain, gate, up):
    group = min(16, lax.axis_size("sp"))
    tp = lax.axis_size("tp")
    rows, width = queries.shape
    dev_rows, model_width = residual_in.shape
    heads = lambdas.shape[0]
    value_dim = width // heads
    vmem = pl.BlockSpec(memory_space=pltpu.VMEM)
    return pl.pallas_call(
        functools.partial(attention_kernel, group, tp),
        name="attend",
        out_shape=(
            jax.ShapeDtypeStruct((dev_rows, model_width), jnp.bfloat16),
            jax.ShapeDtypeStruct((dev_rows, model_width), jnp.bfloat16),
            jax.ShapeDtypeStruct(gate.shape, jnp.bfloat16),
            jax.ShapeDtypeStruct(up.shape, jnp.bfloat16),
        ),
        in_specs=[
            vmem,
            vmem,
            vmem,
            pl.BlockSpec(memory_space=pltpu.SMEM),
            vmem,
            pl.BlockSpec(memory_space=pl.ANY),
            vmem,
            vmem,
            pl.BlockSpec(memory_space=pl.ANY),
            pl.BlockSpec(memory_space=pl.ANY),
        ],
        out_specs=(
            vmem,
            vmem,
            pl.BlockSpec(memory_space=pl.ANY),
            pl.BlockSpec(memory_space=pl.ANY),
        ),
        scratch_shapes=[
            pltpu.VMEM((group, rows, width), jnp.bfloat16),
            pltpu.VMEM((group, rows, width), jnp.bfloat16),
            pltpu.VMEM((2 * heads, rows, value_dim), jnp.bfloat16),
            pltpu.VMEM((2 * heads, rows, 128), jnp.float32),
            pltpu.VMEM((2 * heads, rows, 128), jnp.float32),
            pltpu.VMEM((2 * heads, rows, value_dim), jnp.float32),
            pltpu.VMEM((rows, width), jnp.bfloat16),
            pltpu.VMEM((tp, dev_rows, width), jnp.bfloat16),
            pltpu.VMEM(w_out.shape, jnp.bfloat16),
            pltpu.SemaphoreType.DMA((2, group)),
            pltpu.SemaphoreType.DMA((2, group)),
            pltpu.SemaphoreType.DMA((tp,)),
            pltpu.SemaphoreType.DMA((tp,)),
            pltpu.SemaphoreType.DMA((3,)),
            pltpu.SemaphoreType.DMA((2,)),
            pltpu.SemaphoreType.DMA((2,)),
        ],
        compiler_params=pltpu.CompilerParams(
            collective_id=0, has_side_effects=True, vmem_limit_bytes=VMEM_BYTES
        ),
        cost_estimate=pl.CostEstimate(
            flops=50_000_000_000, bytes_accessed=16_000_000, transcendentals=8_000_000
        ),
    )(
        queries,
        keys,
        values,
        lambdas,
        head_gain.reshape(1, -1),
        w_out,
        residual_in,
        norm_gain.reshape(1, -1),
        gate,
        up,
    )


def expert_kernel(
    group,
    x_ref,
    carried_ref,
    share_ref,
    gate_ref,
    up_ref,
    down_ref,
    far_gate_ref,
    far_up_ref,
    out_ref,
    x_slots,
    share_slots,
    gates,
    ups,
    downs,
    hidden,
    parts,
    sums_in,
    sums_out,
    send_sems,
    recv_sems,
    sum_send,
    sum_recv,
    load_sems,
    weight_send,
    weight_recv,
):
    rows, width = x_ref.shape
    pieces = gates.shape[0]
    half_rows, half_width = rows // 2, width // 2
    last, half = group - 1, group // 2
    right, left = ring_neighbours(group)
    expert = lax.axis_index("sp")
    me_tp = lax.axis_index("tp")
    near = me_tp + 1 - 2 * lax.rem(me_tp, 2)
    far = lax.rem(me_tp + pieces // 2, pieces)

    barrier = pltpu.get_barrier_semaphore()
    for neighbour in (right, left):
        pl.semaphore_signal(barrier, inc=1, device_id={"sp": neighbour}, device_id_type=MESH)
    for neighbour in (near, far):
        pl.semaphore_signal(barrier, inc=1, device_id={"tp": neighbour}, device_id_type=MESH)
    pl.semaphore_wait(barrier, 4)

    def landing(slot, which):
        return share_slots.at[slot] if which == 2 else x_slots.at[slot, which]

    def send(source, slot, which, target):
        return pltpu.make_async_remote_copy(
            src_ref=source,
            dst_ref=landing(slot, which),
            send_sem=send_sems.at[which, slot],
            recv_sem=recv_sems.at[which, slot],
            device_id={"sp": target},
            device_id_type=MESH,
        )

    def weight_send_to(source, target_ref, index, target):
        return pltpu.make_async_remote_copy(
            src_ref=source,
            dst_ref=target_ref,
            send_sem=weight_send.at[index],
            recv_sem=weight_recv.at[index],
            device_id={"tp": target},
            device_id_type=MESH,
        )

    own = (x_ref.at[pl.ds(0, half_rows)], x_ref.at[pl.ds(half_rows, half_rows)], share_ref)
    for which in range(3):
        send(own[which], 1, which, right).start()
        send(own[which], 2, which, left).start()
    far_down = weight_send_to(down_ref, downs.at[2], 5, far)
    far_down.start()
    near_copies = [
        weight_send_to(gate_ref, gates.at[1], 0, near),
        weight_send_to(far_gate_ref, gates.at[3], 1, near),
        weight_send_to(up_ref, ups.at[1], 2, near),
        weight_send_to(far_up_ref, ups.at[3], 3, near),
        weight_send_to(down_ref, downs.at[1], 4, near),
    ]
    loads = [
        pltpu.make_async_copy(gate_ref, gates.at[0], load_sems.at[0]),
        pltpu.make_async_copy(up_ref, ups.at[0], load_sems.at[1]),
        pltpu.make_async_copy(far_gate_ref, gates.at[2], load_sems.at[2]),
        pltpu.make_async_copy(far_up_ref, ups.at[2], load_sems.at[3]),
        pltpu.make_async_copy(down_ref, downs.at[0], load_sems.at[4]),
    ]
    for copy in near_copies + loads:
        copy.start()
    def make_hidden(x, begin):
        def one_piece(piece, unused):
            gate_proj = jnp.dot(x, gates[piece], preferred_element_type=jnp.float32)
            up_proj = jnp.dot(x, ups[piece], preferred_element_type=jnp.float32)
            silu = gate_proj / (1.0 + jnp.exp(-gate_proj))
            hidden[piece, begin : begin + x.shape[0]] = (silu * up_proj).astype(jnp.bfloat16)
            return unused

        lax.fori_loop(0, pieces, one_piece, 0)

    def share_column(share):
        wanted = lax.broadcasted_iota(jnp.int32, share.shape, 0) == expert
        line = jnp.sum(jnp.where(wanted, share, 0.0), axis=0, keepdims=True)
        down_index = lax.broadcasted_iota(jnp.int32, (rows, rows), 0)
        across_index = lax.broadcasted_iota(jnp.int32, (rows, rows), 1)
        square = jnp.where(down_index == across_index, jnp.broadcast_to(line, (rows, rows)), 0.0)
        return jnp.sum(square, axis=1, keepdims=True)

    tile = width // 4

    def make_parts(slots):
        begin, count = slots[0] * rows, len(slots) * rows
        columns = [share_column(share_ref[...] if slot == 0 else share_slots[slot]) for slot in slots]
        column = jnp.concatenate(columns, axis=0)

        def one_tile(index, unused):
            at = pl.ds(pl.multiple_of(index * tile, tile), tile)
            total = jnp.zeros((count, tile), jnp.float32)
            for piece in range(pieces):
                total = total + lax.dot_general(
                    hidden[piece, begin : begin + count],
                    downs[piece, at, :],
                    (((1,), (1,)), ((), ())),
                    preferred_element_type=jnp.float32,
                )
            parts[begin : begin + count, at] = total.astype(jnp.bfloat16).astype(jnp.float32) * column
            return unused

        lax.fori_loop(0, 4, one_tile, 0)

    def exchange(step):
        ahead, behind = 2 * step - 1, 2 * step
        for which in range(3):
            send(landing(ahead, which), ahead, which, right).wait_recv()
            if step < half - 1:
                send(landing(ahead, which), ahead + 2, which, right).start()
            elif which != 1:
                send(landing(ahead, which), last, which, right).start()
            send(landing(behind, which), behind, which, left).wait_recv()
            if step < half - 1:
                send(landing(behind, which), behind + 2, which, left).start()
            elif which == 1:
                send(landing(behind, which), last, which, left).start()

    def sum_copy(side, step, chunk):
        return pltpu.make_async_remote_copy(
            src_ref=sums_out.at[side, step, chunk],
            dst_ref=sums_in.at[side, step, chunk],
            send_sem=sum_send.at[side, step, chunk],
            recv_sem=sum_recv.at[side, step, chunk],
            device_id={"sp": left if side else right},
            device_id_type=MESH,
        )

    def part_of(side, slot, chunk):
        begin = slot * rows + chunk * half_rows
        return parts[begin : begin + half_rows, side * half_width : (side + 1) * half_width]

    def sum_step(step):
        for chunk in range(2):
            for side in range(2):
                if step < half:
                    slot = 2 * step - 1 + side
                elif step == half:
                    slot = last
                else:
                    slot = 2 * (group - step) - side
                value = part_of(side, slot, chunk)
                if step > 1:
                    sum_copy(side, step - 1, chunk).wait_recv()
                    value = value + sums_in[side, step - 1, chunk].astype(jnp.float32)
                sums_out[side, step, chunk] = value.astype(jnp.bfloat16)
                sum_copy(side, step, chunk).start()

    def pair_hidden(step):
        pair = jnp.concatenate(
            [x_slots[slot, part] for slot in (2 * step - 1, 2 * step) for part in range(2)], axis=0
        )
        make_hidden(pair, (2 * step - 1) * rows)

    exchange(1)
    for load in loads:
        load.wait()
    for copy in near_copies:
        copy.wait_recv()
    pair_hidden(1)
    if half > 2:
        exchange(2)
        pair_hidden(2)
    far_down.wait_recv()
    near_down = weight_send_to(downs.at[2], downs.at[3], 6, near)
    near_down.start()
    near_down.wait_recv()
    make_parts((1, 2))
    for step in range(3, half):
        exchange(step)
        sum_step(step - 2)
        make_parts((2 * step - 3, 2 * step - 2))
        pair_hidden(step)
    if half > 2:
        sum_step(half - 2)
        make_parts((last - 2, last - 1))
    send(landing(last, 0), last, 0, right).wait_recv()
    send(landing(last, 1), last, 1, left).wait_recv()
    send(landing(last, 2), last, 2, right).wait_recv()
    sum_step(half - 1)
    make_hidden(jnp.concatenate([x_slots[last, 0], x_slots[last, 1]], axis=0), last * rows)
    make_parts((last,))
    for step in range(half, group):
        sum_step(step)
        if step == half:
            make_hidden(x_ref[...], 0)
        if step == min(half + 1, last):
            make_parts((0,))
    for chunk in range(2):
        here = slice(chunk * half_rows, (chunk + 1) * half_rows)
        for side in range(2):
            there = slice(side * half_width, (side + 1) * half_width)
            sum_copy(side, last, chunk).wait_recv()
            out_ref[here, there] = (
                carried_ref[here, there].astype(jnp.float32)
                + (part_of(side, 0, chunk) + sums_in[side, last, chunk].astype(jnp.float32))
            ).astype(jnp.bfloat16)
    for slot in range(1, group):
        for which in range(3):
            send(landing(slot, which), slot, which, right).wait_send()
    for step in range(1, group):
        for side in range(2):
            for chunk in range(2):
                sum_copy(side, step, chunk).wait_send()
    for copy in near_copies + [far_down, near_down]:
        copy.wait_send()


def expert_layer(normed, carried, shares, gate, up, down, far_gate, far_up):
    group = lax.axis_size("sp")
    pieces = lax.axis_size("tp")
    rows, width = normed.shape
    units = gate.shape[1]
    vmem = pl.BlockSpec(memory_space=pltpu.VMEM)
    outside = pl.BlockSpec(memory_space=pl.ANY)
    bf16 = jnp.bfloat16
    return pl.pallas_call(
        functools.partial(expert_kernel, group),
        name="experts",
        out_shape=jax.ShapeDtypeStruct((rows, width), bf16),
        in_specs=[vmem] * 3 + [outside] * 5,
        out_specs=vmem,
        scratch_shapes=[
            pltpu.VMEM((group, 2, rows // 2, width), bf16),
            pltpu.VMEM((group,) + shares.shape, jnp.float32),
            pltpu.VMEM((pieces, width, units), bf16),
            pltpu.VMEM((pieces, width, units), bf16),
            pltpu.VMEM((pieces, width, units), bf16),
            pltpu.VMEM((pieces, group * rows, units), bf16),
            pltpu.VMEM((group * rows, width), jnp.float32),
            pltpu.VMEM((2, group, 2, rows // 2, width // 2), bf16),
            pltpu.VMEM((2, group, 2, rows // 2, width // 2), bf16),
            pltpu.SemaphoreType.DMA((3, group)),
            pltpu.SemaphoreType.DMA((3, group)),
            pltpu.SemaphoreType.DMA((2, group, 2)),
            pltpu.SemaphoreType.DMA((2, group, 2)),
            pltpu.SemaphoreType.DMA((5,)),
            pltpu.SemaphoreType.DMA((7,)),
            pltpu.SemaphoreType.DMA((7,)),
        ],
        compiler_params=pltpu.CompilerParams(
            collective_id=1, has_side_effects=True, vmem_limit_bytes=VMEM_BYTES
        ),
    )(normed, carried, shares, gate, up, down, far_gate, far_up)


def nearest_first(position, count, nth):
    order = [
        sorted(range(count), key=lambda other: (abs(other - here), other if 2 * here < count else -other))
        for here in range(count)
    ]
    chosen = jnp.int32(order[0][nth])
    for here in range(1, count):
        chosen = jnp.where(position == here, order[here][nth], chosen)
    return chosen


class WeightFlow:
    def __init__(self, chunks, refs, pieces, send_sems, recv_sems, load_sems):
        gate_ref, up_ref, down_ref = refs
        gates, ups, downs = pieces
        me_tp, tp = lax.axis_index("tp"), lax.axis_size("tp")
        near = me_tp + 1 - 2 * lax.rem(me_tp, 2)
        far = lax.rem(me_tp + tp // 2, tp)
        width = gate_ref.shape[0]
        half, tile = width // 2, width // chunks
        self.used = 0

        def to(target, source, landing):
            index = self.used
            self.used += 1
            return pltpu.make_async_remote_copy(
                src_ref=source,
                dst_ref=landing,
                send_sem=send_sems.at[index],
                recv_sem=recv_sems.at[index],
                device_id={"tp": target},
                device_id_type=MESH,
            )

        cuts = [(0, pl.ds(0, width)), (1, pl.ds(0, half)), (1, pl.ds(half, half))]
        cuts += [(2, pl.ds(chunk * tile, tile)) for chunk in range(chunks)]
        self.far = [to(far, refs[kind].at[at], pieces[kind].at[2, at]) for kind, at in cuts]
        self.relays = [to(near, pieces[kind].at[2, at], pieces[kind].at[3, at]) for kind, at in cuts]
        self.near = [to(near, refs[kind], pieces[kind].at[1]) for kind in range(3)]
        self.loads = [
            pltpu.make_async_copy(refs[kind], pieces[kind].at[0], load_sems.at[kind])
            for kind in range(3)
        ]

    def start_far(self, phase):
        if phase == 0:
            for copy in self.far[:2]:
                copy.start()
        else:
            for copy in self.far[2:] + self.near + self.loads:
                copy.start()
            for far, relay in zip(self.far[:2], self.relays[:2]):
                far.wait_recv()
                relay.start()

    def hidden_ready(self):
        self.far[2].wait_recv()
        self.relays[2].start()
        for copy in self.loads:
            copy.wait()
        for copy in self.near + self.relays[:3]:
            copy.wait_recv()

    def down_ready(self, chunk):
        self.far[3 + chunk].wait_recv()
        self.relays[3 + chunk].start()
        self.relays[3 + chunk].wait_recv()

    def finish(self):
        for copy in self.far + self.relays + self.near:
            copy.wait_send()


def attention_part(
    sides,
    cores,
    start_far,
    q_ref,
    k_ref,
    v_ref,
    lam_ref,
    gain_ref,
    w_out_ref,
    residual_ref,
    norm_gain_ref,
    carried_ref,
    normed_ref,
    q_here,
    kv,
    q_masked,
    peaks,
    totals,
    numerators,
    made,
    came,
    lam_all,
    w_out_here,
    in_send,
    q_recv,
    kv_recv,
    pair_send,
    side_send,
    lam_sems,
    row_send,
    row_recv,
    load_sems,
):
    rows, width = q_ref.shape
    depth = kv.shape[2]
    heads = width // 128
    value_dim = width // heads
    head_dim = value_dim // 2
    half = rows // cores
    exponent_scale = head_dim ** (-0.5) * math.log2(math.e)
    me_sp, me_tp = lax.axis_index("sp"), lax.axis_index("tp")
    tp = lax.axis_size("tp")
    z, y = lax.div(me_sp, sides), lax.rem(me_sp, sides)
    x, c = lax.div(me_tp, cores), lax.rem(me_tp, cores)
    other_y, other_c = 1 - y, 1 - c

    def device(at_z, at_y, at_x, at_c):
        return {"sp": at_z * sides + at_y, "tp": at_x * cores + at_c}

    lam_row = lax.broadcasted_iota(jnp.int32, lam_all.shape[1:], 0)
    lam_block = jnp.zeros(lam_all.shape[1:], jnp.float32)
    for head in range(heads):
        lam_block = jnp.where(lam_row == head, lam_ref[head], lam_block)
    lam_all[c] = lam_block

    barrier = pltpu.get_barrier_semaphore()
    plane = depth * tp
    spot = z * tp + me_tp
    for step in range(1, plane):
        peer = lax.rem(spot + step, plane)
        pl.semaphore_signal(
            barrier,
            inc=1,
            device_id={"sp": lax.div(peer, tp) * sides + y, "tp": lax.rem(peer, tp)},
            device_id_type=MESH,
        )
    pl.semaphore_signal(barrier, inc=1, device_id=device(z, other_y, x, c), device_id_type=MESH)
    pl.semaphore_wait(barrier, plane)

    def remote(source, landing, send_sem, recv_sem, target):
        return pltpu.make_async_remote_copy(
            src_ref=source,
            dst_ref=landing,
            send_sem=send_sem,
            recv_sem=recv_sem,
            device_id=target,
            device_id_type=MESH,
        )

    def deliver(source, landing, send_sem, recv_sem, target, stays):
        @pl.when(stays)
        def _():
            pltpu.make_async_copy(source, landing, recv_sem).start()

        @pl.when(jnp.logical_not(stays))
        def _():
            remote(source, landing, send_sem, recv_sem, target).start()

    def left(source, landing, send_sem, recv_sem, target, stays):
        @pl.when(jnp.logical_not(stays))
        def _():
            remote(source, landing, send_sem, recv_sem, target).wait_send()

    inputs = []
    for head in range(heads):
        columns = slice(head * value_dim, (head + 1) * value_dim)
        to_z = c * heads + head
        for core in range(cores):
            inputs.append(
                (
                    q_ref.at[core * half : (core + 1) * half, columns],
                    q_here.at[z],
                    in_send.at[head, core],
                    q_recv.at[z],
                    device(to_z, y, x, core),
                    jnp.logical_and(to_z == z, c == core),
                )
            )
    for head in range(heads):
        columns = slice(head * value_dim, (head + 1) * value_dim)
        to_z = c * heads + head
        for core, source in ((0, k_ref), (1, v_ref)):
            inputs.append(
                (
                    source.at[:, columns],
                    kv.at[core, y, z],
                    in_send.at[head, cores + core],
                    kv_recv.at[core, y, z],
                    device(to_z, y, x, core),
                    jnp.logical_and(to_z == z, c == core),
                )
            )
    lam_copy = remote(lam_all.at[c], lam_all.at[c], lam_sems.at[0], lam_sems.at[1], device(z, y, x, other_c))
    for item in inputs:
        deliver(*item)
    lam_copy.start()
    start_far(0)
    load_w_out = pltpu.make_async_copy(w_out_ref, w_out_here, load_sems.at[0])
    load_w_out.start()

    peaks[...] = jnp.full(peaks.shape, FLOOR_SCORE, jnp.float32)
    totals[...] = jnp.zeros(totals.shape, jnp.float32)
    numerators[...] = jnp.zeros(numerators.shape, jnp.float32)

    def block_wait(tensor, side, at):
        slot = kv.at[tensor, side, at]
        remote(
            slot, slot, pair_send.at[0, 0], kv_recv.at[tensor, side, at], device(z, other_y, x, c)
        ).wait_recv()

    def to_pair(side, at):
        slot = kv.at[c, side, at]
        return remote(
            slot, slot, pair_send.at[side, at], kv_recv.at[c, side, at], device(z, y, x, other_c)
        )

    def to_side(at):
        slot = kv.at[c, y, at]
        return remote(
            slot, slot, side_send.at[at], kv_recv.at[c, y, at], device(z, other_y, x, c)
        )

    def take_own(at):
        block_wait(c, y, at)
        to_side(at).start()
        to_pair(y, at).start()

    def take_side(at):
        block_wait(c, other_y, at)
        to_pair(other_y, at).start()

    def absorb(side, at):
        block_wait(other_c, side, at)
        key_block = kv[0, side, at]
        value_block = kv[1, side, at]
        with_ones = jnp.concatenate([value_block, jnp.ones((rows, 128), jnp.bfloat16)], axis=1)
        for part in range(2):
            for begin in range(0, depth * half, half):
                here = slice(begin, begin + half)
                scores = lax.dot_general(
                    q_masked[part, here],
                    key_block,
                    (((1,), (1,)), ((), ())),
                    preferred_element_type=jnp.float32,
                )
                old_peak = peaks[part, here][:, :1]
                new_peak = jnp.maximum(old_peak, jnp.max(scores, axis=1, keepdims=True))
                weights = jnp.exp2((scores - new_peak) * exponent_scale)
                shrink = jnp.exp2((old_peak - new_peak) * exponent_scale)
                product = jnp.dot(
                    weights.astype(jnp.bfloat16), with_ones, preferred_element_type=jnp.float32
                )
                numerators[part, here] = numerators[part, here] * shrink + product[:, :value_dim]
                totals[part, here] = totals[part, here] * shrink + product[:, value_dim:]
                peaks[part, here] = jnp.broadcast_to(new_peak, (half, 128))

    take_own(z)
    lane = lax.broadcasted_iota(jnp.int32, (half, value_dim), 1)
    for at in range(depth):
        remote(
            q_here.at[at], q_here.at[at], pair_send.at[0, 0], q_recv.at[at], device(z, other_y, x, c)
        ).wait_recv()
        both = q_here[at]
        here = slice(at * half, (at + 1) * half)
        q_masked[0, here] = jnp.where(lane < head_dim, both, jnp.zeros_like(both))
        q_masked[1, here] = jnp.where(lane >= head_dim, both, jnp.zeros_like(both))

    def nth(index):
        chosen = nearest_first(z, depth, 0)
        for place in range(1, depth):
            chosen = jnp.where(index == place, nearest_first(z, depth, place), chosen)
        return chosen

    def one_block(index, unused):
        at = nth(index)
        absorb(y, at)
        take_side(at)

        @pl.when(index < depth - 1)
        def _():
            take_own(nth(index + 1))

        absorb(other_y, at)
        return unused

    lax.fori_loop(0, depth, one_block, 0)

    lam_copy.wait_recv()
    lam_here = lam_all[lax.div(z, heads)]
    lam = jnp.sum(jnp.where(lam_row == lax.rem(z, heads), lam_here, 0.0), axis=0, keepdims=True)
    gain = gain_ref[...] * OUT_SCALE
    dev_rows = residual_ref.shape[0]
    my_head = x * depth + z

    def row_item(at, part):
        return (
            made.at[at, part * dev_rows : (part + 1) * dev_rows],
            came.at[my_head],
            row_send.at[at, part],
            row_recv.at[my_head],
            device(at, y, c, part),
            jnp.logical_and(at == z, jnp.logical_and(x == c, c == part)),
        )

    for place in reversed(range(depth)):
        at = nearest_first(z, depth, place)
        here = pl.ds(pl.multiple_of(at * half, half), half)
        first = numerators[0, here] / totals[0, here][:, :1]
        second = numerators[1, here] / totals[1, here][:, :1]
        combined = first - lam * second
        mean_square = jnp.mean(combined * combined, axis=1, keepdims=True)
        made[at] = (combined * lax.rsqrt(mean_square + EPSILON) * gain).astype(jnp.bfloat16)
        for part in range(half // dev_rows):
            deliver(*row_item(at, part))
    start_far(1)
    load_w_out.wait()
    for head in range(came.shape[0]):
        remote(
            came.at[head], came.at[head], pair_send.at[0, 0], row_recv.at[head], device(z, other_y, x, c)
        ).wait_recv()
    attended = jnp.concatenate([came[head] for head in range(came.shape[0])], axis=1)
    mixed = jnp.dot(attended, w_out_here[...], preferred_element_type=jnp.float32).astype(
        jnp.bfloat16
    )
    carried = (residual_ref[...].astype(jnp.float32) + mixed.astype(jnp.float32)).astype(
        jnp.bfloat16
    )
    carried_ref[...] = carried
    wide = carried.astype(jnp.float32)
    spread = jnp.mean(wide * wide, axis=1, keepdims=True)
    normed_ref[...] = (wide * lax.rsqrt(spread + EPSILON) * norm_gain_ref[...]).astype(
        jnp.bfloat16
    )

    def finish():
        for item in inputs:
            left(*item)
        lam_copy.wait_send()
        for at in range(depth):
            to_side(at).wait_send()
            to_pair(0, at).wait_send()
            to_pair(1, at).wait_send()
            for part in range(half // dev_rows):
                left(*row_item(at, part))

    return finish


def expert_part(
    sides,
    weights,
    x_ref,
    carried_ref,
    share_ref,
    out_ref,
    x_all,
    share_all,
    selections,
    columns,
    picked,
    packed_out,
    gates,
    ups,
    downs,
    hidden,
    results_out,
    results_in,
    results_own,
    parts,
    sums_in,
    sums_out,
    x_send,
    x_recv,
    share_send,
    share_recv,
    pack_send,
    pack_recv,
    result_send,
    result_recv,
    sum_send,
    sum_recv,
):
    rows, width = x_ref.shape
    depth = x_all.shape[0]
    capacity = rows // 2
    pieces = gates.shape[0]
    chunks = x_recv.shape[1]
    tile = width // chunks
    me_sp, me_tp = lax.axis_index("sp"), lax.axis_index("tp")
    z, y = lax.div(me_sp, sides), lax.rem(me_sp, sides)
    partner = z * sides + 1 - y
    has_below, has_above = z > 0, z < depth - 1
    middle = jnp.logical_and(has_below, has_above)
    blocks = [nearest_first(z, depth, place) for place in range(depth)]

    def remote(source, landing, send_sem, recv_sem, target):
        return pltpu.make_async_remote_copy(
            src_ref=source,
            dst_ref=landing,
            send_sem=send_sem,
            recv_sem=recv_sem,
            device_id=target,
            device_id_type=MESH,
        )

    below, above = {"sp": me_sp - sides}, {"sp": me_sp + sides}

    def cut(chunk):
        return pl.ds(chunk * tile, tile)

    def x_copy(source, block, chunk, downward):
        return remote(
            source.at[:, cut(chunk)],
            x_all.at[block, :, cut(chunk)],
            x_send.at[downward, block, chunk],
            x_recv.at[block, chunk],
            below if downward else above,
        )

    def share_copy(source, block, downward):
        return remote(
            source,
            share_all.at[block],
            share_send.at[downward, block],
            share_recv.at[block],
            below if downward else above,
        )

    for downward, exists in ((0, has_above), (1, has_below)):

        @pl.when(exists)
        def _():
            share_copy(share_ref, z, downward).start()
            for chunk in range(chunks):
                x_copy(x_ref, z, chunk, downward).start()

    def to_far(index, source, landing):
        return remote(source, landing, weight_send.at[index], weight_recv.at[index], {"tp": far})

    def to_near(index, source, landing):
        return remote(source, landing, weight_send.at[index], weight_recv.at[index], {"tp": near})

    def select(step, share):
        named = (share > 0.0).astype(jnp.float32)
        earlier = lax.broadcasted_iota(jnp.int32, (rows, rows), 0) < lax.broadcasted_iota(
            jnp.int32, (rows, rows), 1
        )
        rank = jnp.dot(
            named.astype(jnp.bfloat16),
            earlier.astype(jnp.float32).astype(jnp.bfloat16),
            preferred_element_type=jnp.float32,
        )
        expert_row = lax.broadcasted_iota(jnp.int32, share.shape, 0)
        slot = lax.broadcasted_iota(jnp.int32, (capacity, rows), 0).astype(jnp.float32)
        diagonal = lax.broadcasted_iota(jnp.int32, (rows, rows), 0) == lax.broadcasted_iota(
            jnp.int32, (rows, rows), 1
        )
        found = []
        for side, expert in enumerate((partner, me_sp)):

            def line(table):
                return jnp.sum(jnp.where(expert_row == expert, table, 0.0), axis=0, keepdims=True)

            taken = jnp.where(jnp.logical_and(slot == line(rank), line(named) > 0.0), 1.0, 0.0)
            found.append(taken)
            selections[step, side] = taken.T.astype(jnp.bfloat16)
            square = jnp.where(diagonal, jnp.broadcast_to(line(share), (rows, rows)), 0.0)
            columns[step, side] = jnp.broadcast_to(
                jnp.sum(square, axis=1, keepdims=True), (rows, 128)
            )
        return jnp.concatenate(found, axis=0).astype(jnp.bfloat16)

    def pack_copy(step, chunk):
        return remote(
            packed_out.at[step, :, cut(chunk)],
            picked.at[pl.ds(step * rows, capacity), cut(chunk)],
            pack_send.at[step, chunk],
            pack_recv.at[step, chunk],
            {"sp": partner},
        )

    def pack(step, take, chunk):
        block = x_ref[:, cut(chunk)] if step == 0 else x_all[blocks[step], :, cut(chunk)]
        compact = jnp.dot(take, block, preferred_element_type=jnp.float32).astype(jnp.bfloat16)
        packed_out[step, :, cut(chunk)] = compact[:capacity]
        picked[step * rows + capacity : (step + 1) * rows, cut(chunk)] = compact[capacity:]
        pack_copy(step, chunk).start()

    def forward(step, chunk):
        block = blocks[step]
        go_up = jnp.logical_and(block < z, has_above)
        go_down = jnp.logical_and(block > z, has_below)
        if chunk == 0:
            share_copy(share_all.at[block], block, 0).wait_recv()
        x_copy(x_all.at[block], block, chunk, 0).wait_recv()
        for downward, goes in ((0, go_up), (1, go_down)):

            @pl.when(goes)
            def _():
                if chunk == 0:
                    share_copy(share_all.at[block], block, downward).start()
                x_copy(x_all.at[block], block, chunk, downward).start()

    def chosen(step):
        return select(step, share_ref[...] if step == 0 else share_all[blocks[step]])

    def pack_all(step):
        take = chosen(step)
        for chunk in range(chunks):
            pack(step, take, chunk)

    def bring(step):
        forward(step, 0)
        take = chosen(step)
        pack(step, take, 0)
        for chunk in range(1, chunks):
            forward(step, chunk)
            pack(step, take, chunk)

    def make_hidden(first, last, piece):
        here = slice(first * rows, last * rows)
        x = picked[here]
        gate_proj = jnp.dot(x, gates[piece], preferred_element_type=jnp.float32)
        up_proj = jnp.dot(x, ups[piece], preferred_element_type=jnp.float32)
        silu = gate_proj / (1.0 + jnp.exp(-gate_proj))
        hidden[piece, here] = (silu * up_proj).astype(jnp.bfloat16)

    def result_copy(step, chunk):
        return remote(
            results_out.at[step, :, cut(chunk)],
            results_in.at[step, :, cut(chunk)],
            result_send.at[step, chunk],
            result_recv.at[step, chunk],
            {"sp": partner},
        )

    def make_results(first, last, chunk):
        total = jnp.zeros(((last - first) * rows, tile), jnp.float32)
        for piece in range(pieces):
            total = total + lax.dot_general(
                hidden[piece, first * rows : last * rows],
                downs[piece, cut(chunk)],
                (((1,), (1,)), ((), ())),
                preferred_element_type=jnp.float32,
            )
        total = total.astype(jnp.bfloat16)
        for step in range(first, last):
            at = (step - first) * rows
            results_out[step, :, cut(chunk)] = total[at : at + capacity]
            results_own[step, :, cut(chunk)] = total[at + capacity : at + rows]
            result_copy(step, chunk).start()

    def spread(step, chunk):
        result_copy(step, chunk).wait_recv()
        theirs = jnp.dot(
            selections[step, 0], results_in[step, :, cut(chunk)], preferred_element_type=jnp.float32
        )
        ours = jnp.dot(
            selections[step, 1], results_own[step, :, cut(chunk)], preferred_element_type=jnp.float32
        )
        parts[step, :, cut(chunk)] = theirs * columns[step, 0][:, :1] + ours * columns[step, 1][:, :1]

    def sum_copy(step, chunk, downward):
        block = blocks[step]
        return remote(
            sums_out.at[step, :, cut(chunk)],
            sums_in.at[downward, block, :, cut(chunk)],
            sum_send.at[step, chunk],
            sum_recv.at[downward, block, chunk],
            below if downward else above,
        )

    def pass_sum(step, chunk, has_outer):
        block = blocks[step]
        for downward, goes in ((0, block > z), (1, block < z)):

            @pl.when(goes)
            def _():
                value = parts[step, :, cut(chunk)]
                if has_outer:
                    sum_copy(step, chunk, downward).wait_recv()
                    value = value + sums_in[downward, block, :, cut(chunk)].astype(jnp.float32)
                sums_out[step, :, cut(chunk)] = value.astype(jnp.bfloat16)
                sum_copy(step, chunk, downward).start()

    def at_end(action):
        pl.when(jnp.logical_not(middle))(action)

    def at_middle(action):
        pl.when(middle)(action)

    pack_all(0)
    forward(1, 0)
    first_take = chosen(1)
    pack(1, first_take, 0)
    at_middle(functools.partial(forward, 2, 0))
    for chunk in range(1, chunks):
        forward(1, chunk)
        pack(1, first_take, chunk)
        at_middle(functools.partial(forward, 2, chunk))
    at_middle(functools.partial(pack_all, 2))

    def packed(step):
        for chunk in range(chunks):
            pack_copy(step, chunk).wait_recv()

    def all_hidden(step):
        for piece in range(pieces):
            make_hidden(step, step + 1, piece)

    def settle(step, chunk):
        spread(step, chunk)
        at_end(functools.partial(pass_sum, step, chunk, False))

    weights.hidden_ready()
    packed(1)
    all_hidden(1)
    early, late = range(chunks // 2), range(chunks // 2, chunks)
    for chunk in early:
        weights.down_ready(chunk)
        make_results(1, 2, chunk)
    at_end(functools.partial(bring, 2))
    at_middle(functools.partial(bring, 3))
    for chunk in early:
        settle(1, chunk)
    packed(2)
    all_hidden(2)
    for chunk in early:
        make_results(2, 3, chunk)
    for chunk in late:
        weights.down_ready(chunk)
        make_results(1, 3, chunk)
    for chunk in late:
        settle(1, chunk)
    packed(0)
    all_hidden(0)
    for chunk in range(chunks):
        settle(2, chunk)
    at_end(functools.partial(bring, 3))
    packed(3)
    all_hidden(3)
    for chunk in range(chunks):
        make_results(3, 4, chunk)
    for chunk in range(chunks):
        make_results(0, 1, chunk)
    for chunk in range(chunks):
        at_middle(functools.partial(pass_sum, 2, chunk, True))
    for chunk in range(chunks):
        spread(3, chunk)
        at_end(functools.partial(pass_sum, 3, chunk, False))

        @at_middle
        def _():
            pass_sum(3, chunk, True)
            pass_sum(1, chunk, True)

    for chunk in range(chunks):
        spread(0, chunk)
    for chunk in range(chunks):
        here = cut(chunk)

        def arrived(downward):
            landing = sums_in.at[downward, z, :, here]
            remote(
                landing, landing, sum_send.at[0, chunk], sum_recv.at[downward, z, chunk], above
            ).wait_recv()
            parts[0, :, here] = parts[0, :, here] + sums_in[downward, z, :, here].astype(jnp.float32)

        pl.when(has_below)(functools.partial(arrived, 0))
        pl.when(has_above)(functools.partial(arrived, 1))
        out_ref[:, here] = (carried_ref[:, here].astype(jnp.float32) + parts[0, :, here]).astype(
            jnp.bfloat16
        )

    for downward, exists in ((0, has_above), (1, has_below)):

        @pl.when(exists)
        def _():
            share_copy(share_ref, z, downward).wait_send()
            for chunk in range(chunks):
                x_copy(x_ref, z, chunk, downward).wait_send()

    for step in range(1, depth):
        block = blocks[step]
        for downward, goes in (
            (0, jnp.logical_and(block < z, has_above)),
            (1, jnp.logical_and(block > z, has_below)),
        ):

            @pl.when(goes)
            def _():
                share_copy(share_all.at[block], block, downward).wait_send()
                for chunk in range(chunks):
                    x_copy(x_all.at[block], block, chunk, downward).wait_send()

    for step in range(depth):
        for chunk in range(chunks):
            pack_copy(step, chunk).wait_send()
            result_copy(step, chunk).wait_send()
            if step:
                sum_copy(step, chunk, 0).wait_send()


def layer_kernel(sides, cores, chunks, *refs):
    inputs, rest = refs[:8], refs[8:]
    share_ref, gate_ref, up_ref, down_ref, out_ref = rest[:5]
    carried, normed = rest[5:7]
    attention_scratch, rest = rest[7:26], rest[26:]
    expert_scratch, (weight_send, weight_recv, weight_loads) = rest[:-3], rest[-3:]
    weights = WeightFlow(
        chunks,
        (gate_ref, up_ref, down_ref),
        expert_scratch[6:9],
        weight_send,
        weight_recv,
        weight_loads,
    )
    finish = attention_part(
        sides, cores, weights.start_far, *inputs, carried, normed, *attention_scratch
    )
    expert_part(sides, weights, normed, carried, share_ref, out_ref, *expert_scratch)
    finish()
    weights.finish()


def whole_layer(
    queries, keys, values, lambdas, head_gain, w_out, residual_in, norm_gain, shares, gate, up, down
):
    tp = lax.axis_size("tp")
    sides, cores, chunks = 2, 2, 4
    depth = lax.axis_size("sp") // sides
    rows, width = queries.shape
    dev_rows, model_width = residual_in.shape
    units = gate.shape[1]
    value_dim = 128
    heads_all = (width // value_dim) * tp
    half = rows // cores
    capacity = dev_rows // 2
    vmem = pl.BlockSpec(memory_space=pltpu.VMEM)
    smem = pl.BlockSpec(memory_space=pltpu.SMEM)
    outside = pl.BlockSpec(memory_space=pl.ANY)
    bf16, f32 = jnp.bfloat16, jnp.float32
    dma = pltpu.SemaphoreType.DMA
    attention_scratch = [
        pltpu.VMEM((depth, half, value_dim), bf16),
        pltpu.VMEM((2, sides, depth, rows, value_dim), bf16),
        pltpu.VMEM((2, depth * half, value_dim), bf16),
        pltpu.VMEM((2, depth * half, 128), f32),
        pltpu.VMEM((2, depth * half, 128), f32),
        pltpu.VMEM((2, depth * half, value_dim), f32),
        pltpu.VMEM((depth, half, value_dim), bf16),
        pltpu.VMEM((heads_all, dev_rows, value_dim), bf16),
        pltpu.VMEM((cores, 8, 128), f32),
        pltpu.VMEM(w_out.shape, bf16),
        dma((width // value_dim, 2 * cores)),
        dma((depth,)),
        dma((2, sides, depth)),
        dma((sides, depth)),
        dma((depth,)),
        dma((2,)),
        dma((depth, half // dev_rows)),
        dma((heads_all,)),
        dma((1,)),
    ]
    expert_scratch = [
        pltpu.VMEM((depth, dev_rows, model_width), bf16),
        pltpu.VMEM((depth,) + shares.shape, f32),
        pltpu.VMEM((depth, 2, dev_rows, capacity), bf16),
        pltpu.VMEM((depth, 2, dev_rows, 128), f32),
        pltpu.VMEM((depth * dev_rows, model_width), bf16),
        pltpu.VMEM((depth, capacity, model_width), bf16),
        pltpu.VMEM((tp, model_width, units), bf16),
        pltpu.VMEM((tp, model_width, units), bf16),
        pltpu.VMEM((tp, model_width, units), bf16),
        pltpu.VMEM((tp, depth * dev_rows, units), bf16),
        pltpu.VMEM((depth, capacity, model_width), bf16),
        pltpu.VMEM((depth, capacity, model_width), bf16),
        pltpu.VMEM((depth, capacity, model_width), bf16),
        pltpu.VMEM((depth, dev_rows, model_width), f32),
        pltpu.VMEM((2, depth, dev_rows, model_width), bf16),
        pltpu.VMEM((depth, dev_rows, model_width), bf16),
        dma((2, depth, chunks)),
        dma((depth, chunks)),
        dma((2, depth)),
        dma((depth,)),
        dma((depth, chunks)),
        dma((depth, chunks)),
        dma((depth, chunks)),
        dma((depth, chunks)),
        dma((depth, chunks)),
        dma((2, depth, chunks)),
    ]
    weight_copies = 2 * (chunks + 3) + 3
    return pl.pallas_call(
        functools.partial(layer_kernel, sides, cores, chunks),
        name="layer",
        out_shape=jax.ShapeDtypeStruct((dev_rows, model_width), bf16),
        in_specs=[vmem, vmem, vmem, smem, vmem, outside, vmem, vmem, vmem] + [outside] * 3,
        out_specs=vmem,
        scratch_shapes=[
            pltpu.VMEM((dev_rows, model_width), bf16),
            pltpu.VMEM((dev_rows, model_width), bf16),
        ]
        + attention_scratch
        + expert_scratch
        + [dma((weight_copies,)), dma((weight_copies,)), dma((3,))],
        compiler_params=pltpu.CompilerParams(
            collective_id=2, has_side_effects=True, vmem_limit_bytes=VMEM_BYTES
        ),
    )(
        queries,
        keys,
        values,
        lambdas,
        head_gain.reshape(1, -1),
        w_out,
        residual_in,
        norm_gain.reshape(1, -1),
        shares,
        gate,
        up,
        down,
    )


def weight_pieces(weights):
    pieces = [weights]
    for bit in reversed(range(lax.axis_size("tp").bit_length() - 1)):
        pieces = pieces + [
            tuple(swapped(array, "tp", bit) for array in piece) for piece in pieces
        ]
    return pieces


def local(
    queries,
    keys,
    values,
    lambdas,
    head_gain,
    w_out,
    residual_in,
    norm_gain,
    route_ids,
    route_weight,
    w_gate,
    w_up,
    w_down,
):
    sp_size, tp_size = lax.axis_size("sp"), lax.axis_size("tp")
    whole_heads = lambdas.shape[0] * 128 == queries.shape[1]
    square = queries.shape[0] == 2 * 2 * residual_in.shape[0]
    columns_fit = sp_size == 8 and tp_size == 4 and lambdas.shape[0] == 2 and whole_heads and square
    if columns_fit and w_gate.shape[0] == 1:
        named = lax.broadcasted_iota(jnp.int32, (sp_size, residual_in.shape[0], 2), 0)
        shares = jnp.sum(jnp.where(named == route_ids[None], route_weight[None], 0.0), axis=2)
        tensors = (queries, keys, values, lambdas, head_gain, w_out, residual_in, norm_gain)
        return whole_layer(*tensors, shares, w_gate[0], w_up[0], w_down[0])
    carried, normed, far_gate, far_up = attend(
        queries,
        keys,
        values,
        lambdas,
        head_gain,
        w_out,
        residual_in,
        norm_gain,
        w_gate.reshape(-1, w_gate.shape[-1]),
        w_up.reshape(-1, w_up.shape[-1]),
    )
    if w_gate.shape[0] == 1 and 4 <= sp_size <= 8 and tp_size == 4:
        named = lax.broadcasted_iota(jnp.int32, (sp_size, residual_in.shape[0], 2), 0)
        shares = jnp.sum(jnp.where(named == route_ids[None], route_weight[None], 0.0), axis=2)
        return expert_layer(
            normed, carried, shares, w_gate[0], w_up[0], w_down[0], far_gate, far_up
        )
    pieces = weight_pieces((w_gate, w_up, w_down))
    carried_wide = carried.astype(jnp.float32)
    dev_rows = residual_in.shape[0]
    model_width = normed.shape[1]
    experts_here = w_gate.shape[0]
    expert_count = experts_here * lax.axis_size("sp")
    capacity = max(2, 4 * dev_rows // expert_count)
    flat_ids = route_ids.reshape(-1)
    targets = flat_ids * capacity + slot_numbers(flat_ids)
    slot_ids = lax.broadcasted_iota(jnp.int32, (expert_count * capacity, dev_rows, 2), 0)
    placement_matrix = jnp.sum(
        (targets.reshape(1, dev_rows, 2) == slot_ids).astype(jnp.int32), axis=2
    ).astype(jnp.bfloat16)
    outgoing = jnp.dot(placement_matrix, normed, preferred_element_type=jnp.float32).astype(
        jnp.bfloat16
    )
    outgoing = outgoing.reshape(lax.axis_size("sp"), experts_here, capacity, model_width)
    arrived = lax.all_to_all(outgoing, "sp", split_axis=0, concat_axis=0, tiled=True)
    summed = 0.0
    for gate_piece, up_piece, down_piece in pieces:
        gate_proj = jnp.einsum("secd,edf->secf", arrived, gate_piece, preferred_element_type=jnp.float32)
        up_proj = jnp.einsum("secd,edf->secf", arrived, up_piece, preferred_element_type=jnp.float32)
        hidden = (jax.nn.silu(gate_proj) * up_proj).astype(jnp.bfloat16)
        summed = summed + jnp.einsum(
            "secf,edf->secd", hidden, down_piece, preferred_element_type=jnp.float32
        )
    returned = send_back(summed.astype(jnp.bfloat16))
    flat_back = returned.reshape(expert_count * capacity, model_width)
    picked = (
        jnp.take(flat_back, targets, axis=0).astype(jnp.float32).reshape(dev_rows, 2, model_width)
    )
    layer_out = carried_wide + jnp.sum(route_weight[..., None] * picked, axis=1)
    return layer_out.astype(jnp.bfloat16)


def solution(mesh):
    placed = (
        P("sp", "tp"),
        P("sp", "tp"),
        P("sp", "tp"),
        P("tp"),
        P(),
        P(),
        P(("sp", "tp"), None),
        P(),
        P(("sp", "tp"), None),
        P(("sp", "tp"), None),
        P("sp", None, "tp"),
        P("sp", None, "tp"),
        P("sp", None, "tp"),
    )
    return jax.shard_map(
        local, mesh=mesh, in_specs=placed, out_specs=P(("sp", "tp"), None), check_vma=False
    )
```

```python
import functools
import math

import jax
import jax.numpy as jnp
from jax import lax
from jax.experimental import pallas as pl
from jax.experimental.pallas import tpu as pltpu
from jax.sharding import PartitionSpec as P

EPSILON = 1e-06
OUT_SCALE = 0.8
FLOOR_SCORE = -1e30


def swapped(value, axis, distance):
    mask = 2**distance
    pairs = [(source, source ^ mask) for source in range(lax.axis_size(axis))]
    return lax.ppermute(value, axis, pairs)


def slot_numbers(flat_ids):
    count_ids = flat_ids.shape[0]
    positions = lax.broadcasted_iota(jnp.int32, (count_ids, count_ids), 0)
    earlier = lax.broadcasted_iota(jnp.int32, (count_ids, count_ids), 1) < positions
    matches = (flat_ids[:, None] == flat_ids[None, :]) & earlier
    return jnp.sum(matches.astype(jnp.int32), axis=1)


def send_back(results):
    return lax.all_to_all(results, "sp", split_axis=0, concat_axis=0, tiled=True)

MESH = pl.DeviceIdType.MESH
VMEM_BYTES = 60 * 1024 * 1024


def ring_neighbours(group):
    me = lax.axis_index("sp")
    spot = lax.rem(me, group)
    base = me - spot
    even = lax.rem(spot, 2) == 0
    up = jnp.where(even, jnp.where(spot == group - 2, group - 1, spot + 2), jnp.where(spot == 1, 0, spot - 2))
    down = jnp.where(even, jnp.where(spot == 0, 1, spot - 2), jnp.where(spot == group - 1, group - 2, spot + 2))
    return base + up, base + down


def attention_kernel(
    group,
    tp,
    q_ref,
    k_ref,
    v_ref,
    lam_ref,
    gain_ref,
    w_out_ref,
    residual_ref,
    norm_gain_ref,
    gate_ref,
    up_ref,
    carried_ref,
    normed_ref,
    far_gate_ref,
    far_up_ref,
    k_slots,
    v_slots,
    q_masked,
    peaks,
    totals,
    numerators,
    made,
    came,
    w_out_here,
    send_sems,
    recv_sems,
    row_send,
    row_recv,
    load_sems,
    far_send,
    far_recv,
):
    rows = q_ref.shape[0]
    heads = lam_ref.shape[0]
    value_dim = v_ref.shape[1] // heads
    head_dim = value_dim // 2
    exponent_scale = head_dim ** (-0.5) * math.log2(math.e)
    right, left = ring_neighbours(group)
    me_tp = lax.axis_index("tp")

    barrier = pltpu.get_barrier_semaphore()
    for neighbour in (right, left):
        pl.semaphore_signal(barrier, inc=1, device_id={"sp": neighbour}, device_id_type=MESH)
    for step in range(1, tp):
        pl.semaphore_signal(
            barrier, inc=1, device_id={"tp": lax.rem(me_tp + step, tp)}, device_id_type=MESH
        )
    pl.semaphore_wait(barrier, 2 + tp - 1)

    def send(source, slots, which, slot, target):
        return pltpu.make_async_remote_copy(
            src_ref=source,
            dst_ref=slots.at[slot],
            send_sem=send_sems.at[which, slot],
            recv_sem=recv_sems.at[which, slot],
            device_id={"sp": target},
            device_id_type=MESH,
        )

    last = group - 1
    if group > 2:
        for slot, target in ((1, right), (2, left)):
            send(k_ref, k_slots, 0, slot, target).start()
            send(v_ref, v_slots, 1, slot, target).start()
    elif group == 2:
        send(k_ref, k_slots, 0, 1, right).start()
        send(v_ref, v_slots, 1, 1, left).start()
    own_loads = (
        pltpu.make_async_copy(k_ref, k_slots.at[0], load_sems.at[0]),
        pltpu.make_async_copy(v_ref, v_slots.at[0], load_sems.at[1]),
    )
    for load in own_loads:
        load.start()
    load_w_out = pltpu.make_async_copy(w_out_ref, w_out_here, load_sems.at[2])
    load_w_out.start()

    far_copies = [
        pltpu.make_async_remote_copy(
            src_ref=source,
            dst_ref=landing,
            send_sem=far_send.at[index],
            recv_sem=far_recv.at[index],
            device_id={"tp": lax.rem(me_tp + tp // 2, tp)},
            device_id_type=MESH,
        )
        for index, (source, landing) in enumerate(((gate_ref, far_gate_ref), (up_ref, far_up_ref)))
    ]
    for copy in far_copies:
        copy.start()

    lane = lax.broadcasted_iota(jnp.int32, (rows, value_dim), 1)
    for head in range(heads):
        both = q_ref[:, head * value_dim : (head + 1) * value_dim]
        q_masked[2 * head] = jnp.where(lane < head_dim, both, jnp.zeros_like(both))
        q_masked[2 * head + 1] = jnp.where(lane >= head_dim, both, jnp.zeros_like(both))
    peaks[...] = jnp.full(peaks.shape, FLOOR_SCORE, jnp.float32)
    totals[...] = jnp.zeros(totals.shape, jnp.float32)
    numerators[...] = jnp.zeros(numerators.shape, jnp.float32)
    for load in own_loads:
        load.wait()

    chunk = min(rows, 256)

    def absorb(slot, count):
        keys_here = count * k_slots.shape[1]
        for head in range(heads):
            columns = slice(head * value_dim, (head + 1) * value_dim)
            key_block = k_slots[pl.ds(slot, count), :, columns].reshape(keys_here, value_dim)
            value_block = v_slots[pl.ds(slot, count), :, columns].reshape(keys_here, value_dim)
            with_ones = jnp.concatenate(
                [value_block, jnp.ones((keys_here, 128), jnp.bfloat16)], axis=1
            )
            for part in (2 * head, 2 * head + 1):
                for begin in range(0, rows, chunk):
                    here = slice(begin, begin + chunk)
                    scores = lax.dot_general(
                        q_masked[part, here],
                        key_block,
                        (((1,), (1,)), ((), ())),
                        preferred_element_type=jnp.float32,
                    )
                    old_peak = peaks[part, here][:, :1]
                    new_peak = jnp.maximum(old_peak, jnp.max(scores, axis=1, keepdims=True))
                    weights = jnp.exp2((scores - new_peak) * exponent_scale)
                    shrink = jnp.exp2((old_peak - new_peak) * exponent_scale)
                    product = jnp.dot(
                        weights.astype(jnp.bfloat16), with_ones, preferred_element_type=jnp.float32
                    )
                    numerators[part, here] = (
                        numerators[part, here] * shrink + product[:, :value_dim]
                    )
                    totals[part, here] = totals[part, here] * shrink + product[:, value_dim:]
                    peaks[part, here] = jnp.broadcast_to(new_peak, (chunk, 128))

    def one_pair(pair, unused):
        slot = 2 * pair + 1

        def pass_on(which, slots, at, target):
            send(slots.at[at], slots, which, at, target).wait_recv()

            @pl.when(at + 2 <= last - 1)
            def _():
                send(slots.at[at], slots, which, at + 2, target).start()

        for which, slots in ((0, k_slots), (1, v_slots)):
            pass_on(which, slots, slot, right)
            if which == 0:

                @pl.when(slot == last - 2)
                def _():
                    send(slots.at[slot], slots, which, last, right).start()

            pass_on(which, slots, slot + 1, left)
            if which == 1:

                @pl.when(slot == last - 2)
                def _():
                    send(slots.at[slot + 1], slots, which, last, left).start()

        absorb(slot, 2)
        return unused

    absorb(0, 1)
    lax.fori_loop(0, (group - 2) // 2, one_pair, 0)
    if last:
        send(k_slots.at[last], k_slots, 0, last, right).wait_recv()
        send(v_slots.at[last], v_slots, 1, last, left).wait_recv()
        absorb(last, 1)

    gain = gain_ref[...] * OUT_SCALE
    for head in range(heads):
        first = numerators[2 * head] / totals[2 * head][:, :1]
        second = numerators[2 * head + 1] / totals[2 * head + 1][:, :1]
        combined = first - lam_ref[head] * second
        mean_square = jnp.mean(combined * combined, axis=1, keepdims=True)
        made[:, head * value_dim : (head + 1) * value_dim] = (
            combined * lax.rsqrt(mean_square + EPSILON) * gain
        ).astype(jnp.bfloat16)

    dev_rows = residual_ref.shape[0]

    def row_copy(step, owner, target):
        return pltpu.make_async_remote_copy(
            src_ref=made.at[pl.ds(pl.multiple_of(target * dev_rows, dev_rows), dev_rows)],
            dst_ref=came.at[owner],
            send_sem=row_send.at[step],
            recv_sem=row_recv.at[step],
            device_id={"tp": target},
            device_id_type=MESH,
        )

    sends = [row_copy(step, me_tp, lax.rem(me_tp + step, tp)) for step in range(1, tp)]
    for copy in sends:
        copy.start()
    came[me_tp] = made[pl.ds(pl.multiple_of(me_tp * dev_rows, dev_rows), dev_rows)]
    load_w_out.wait()
    for step in range(1, tp):
        row_copy(
            step, lax.rem(me_tp + tp - step, tp), lax.rem(me_tp + step, tp)
        ).wait_recv()
    attended = jnp.concatenate([came[peer] for peer in range(tp)], axis=1)
    mixed = jnp.dot(attended, w_out_here[...], preferred_element_type=jnp.float32).astype(
        jnp.bfloat16
    )
    carried = (residual_ref[...].astype(jnp.float32) + mixed.astype(jnp.float32)).astype(
        jnp.bfloat16
    )
    carried_ref[...] = carried
    wide = carried.astype(jnp.float32)
    spread = jnp.mean(wide * wide, axis=1, keepdims=True)
    normed_ref[...] = (wide * lax.rsqrt(spread + EPSILON) * norm_gain_ref[...]).astype(
        jnp.bfloat16
    )
    for copy in sends:
        copy.wait_send()
    for slot in range(1, group):
        send(k_ref, k_slots, 0, slot, right).wait_send()
        send(v_ref, v_slots, 1, slot, right).wait_send()
    for copy in far_copies:
        copy.wait()


def attend(queries, keys, values, lambdas, head_gain, w_out, residual_in, norm_gain, gate, up):
    group = min(16, lax.axis_size("sp"))
    tp = lax.axis_size("tp")
    rows, width = queries.shape
    dev_rows, model_width = residual_in.shape
    heads = lambdas.shape[0]
    value_dim = width // heads
    vmem = pl.BlockSpec(memory_space=pltpu.VMEM)
    return pl.pallas_call(
        functools.partial(attention_kernel, group, tp),
        name="attend",
        out_shape=(
            jax.ShapeDtypeStruct((dev_rows, model_width), jnp.bfloat16),
            jax.ShapeDtypeStruct((dev_rows, model_width), jnp.bfloat16),
            jax.ShapeDtypeStruct(gate.shape, jnp.bfloat16),
            jax.ShapeDtypeStruct(up.shape, jnp.bfloat16),
        ),
        in_specs=[
            vmem,
            vmem,
            vmem,
            pl.BlockSpec(memory_space=pltpu.SMEM),
            vmem,
            pl.BlockSpec(memory_space=pl.ANY),
            vmem,
            vmem,
            pl.BlockSpec(memory_space=pl.ANY),
            pl.BlockSpec(memory_space=pl.ANY),
        ],
        out_specs=(
            vmem,
            vmem,
            pl.BlockSpec(memory_space=pl.ANY),
            pl.BlockSpec(memory_space=pl.ANY),
        ),
        scratch_shapes=[
            pltpu.VMEM((group, rows, width), jnp.bfloat16),
            pltpu.VMEM((group, rows, width), jnp.bfloat16),
            pltpu.VMEM((2 * heads, rows, value_dim), jnp.bfloat16),
            pltpu.VMEM((2 * heads, rows, 128), jnp.float32),
            pltpu.VMEM((2 * heads, rows, 128), jnp.float32),
            pltpu.VMEM((2 * heads, rows, value_dim), jnp.float32),
            pltpu.VMEM((rows, width), jnp.bfloat16),
            pltpu.VMEM((tp, dev_rows, width), jnp.bfloat16),
            pltpu.VMEM(w_out.shape, jnp.bfloat16),
            pltpu.SemaphoreType.DMA((2, group)),
            pltpu.SemaphoreType.DMA((2, group)),
            pltpu.SemaphoreType.DMA((tp,)),
            pltpu.SemaphoreType.DMA((tp,)),
            pltpu.SemaphoreType.DMA((3,)),
            pltpu.SemaphoreType.DMA((2,)),
            pltpu.SemaphoreType.DMA((2,)),
        ],
        compiler_params=pltpu.CompilerParams(
            collective_id=0, has_side_effects=True, vmem_limit_bytes=VMEM_BYTES
        ),
        cost_estimate=pl.CostEstimate(
            flops=50_000_000_000, bytes_accessed=16_000_000, transcendentals=8_000_000
        ),
    )(
        queries,
        keys,
        values,
        lambdas,
        head_gain.reshape(1, -1),
        w_out,
        residual_in,
        norm_gain.reshape(1, -1),
        gate,
        up,
    )


def expert_kernel(
    group,
    x_ref,
    carried_ref,
    share_ref,
    gate_ref,
    up_ref,
    down_ref,
    far_gate_ref,
    far_up_ref,
    out_ref,
    x_slots,
    share_slots,
    gates,
    ups,
    downs,
    hidden,
    parts,
    sums_in,
    sums_out,
    send_sems,
    recv_sems,
    sum_send,
    sum_recv,
    load_sems,
    weight_send,
    weight_recv,
):
    rows, width = x_ref.shape
    pieces = gates.shape[0]
    half_rows, half_width = rows // 2, width // 2
    last, half = group - 1, group // 2
    right, left = ring_neighbours(group)
    expert = lax.axis_index("sp")
    me_tp = lax.axis_index("tp")
    near = me_tp + 1 - 2 * lax.rem(me_tp, 2)
    far = lax.rem(me_tp + pieces // 2, pieces)

    barrier = pltpu.get_barrier_semaphore()
    for neighbour in (right, left):
        pl.semaphore_signal(barrier, inc=1, device_id={"sp": neighbour}, device_id_type=MESH)
    for neighbour in (near, far):
        pl.semaphore_signal(barrier, inc=1, device_id={"tp": neighbour}, device_id_type=MESH)
    pl.semaphore_wait(barrier, 4)

    def landing(slot, which):
        return share_slots.at[slot] if which == 2 else x_slots.at[slot, which]

    def send(source, slot, which, target):
        return pltpu.make_async_remote_copy(
            src_ref=source,
            dst_ref=landing(slot, which),
            send_sem=send_sems.at[which, slot],
            recv_sem=recv_sems.at[which, slot],
            device_id={"sp": target},
            device_id_type=MESH,
        )

    def weight_send_to(source, target_ref, index, target):
        return pltpu.make_async_remote_copy(
            src_ref=source,
            dst_ref=target_ref,
            send_sem=weight_send.at[index],
            recv_sem=weight_recv.at[index],
            device_id={"tp": target},
            device_id_type=MESH,
        )

    own = (x_ref.at[pl.ds(0, half_rows)], x_ref.at[pl.ds(half_rows, half_rows)], share_ref)
    for which in range(3):
        send(own[which], 1, which, right).start()
        send(own[which], 2, which, left).start()
    far_down = weight_send_to(down_ref, downs.at[2], 5, far)
    far_down.start()
    near_copies = [
        weight_send_to(gate_ref, gates.at[1], 0, near),
        weight_send_to(far_gate_ref, gates.at[3], 1, near),
        weight_send_to(up_ref, ups.at[1], 2, near),
        weight_send_to(far_up_ref, ups.at[3], 3, near),
        weight_send_to(down_ref, downs.at[1], 4, near),
    ]
    loads = [
        pltpu.make_async_copy(gate_ref, gates.at[0], load_sems.at[0]),
        pltpu.make_async_copy(up_ref, ups.at[0], load_sems.at[1]),
        pltpu.make_async_copy(far_gate_ref, gates.at[2], load_sems.at[2]),
        pltpu.make_async_copy(far_up_ref, ups.at[2], load_sems.at[3]),
        pltpu.make_async_copy(down_ref, downs.at[0], load_sems.at[4]),
    ]
    for copy in near_copies + loads:
        copy.start()
    def make_hidden(x, begin):
        def one_piece(piece, unused):
            gate_proj = jnp.dot(x, gates[piece], preferred_element_type=jnp.float32)
            up_proj = jnp.dot(x, ups[piece], preferred_element_type=jnp.float32)
            silu = gate_proj / (1.0 + jnp.exp(-gate_proj))
            hidden[piece, begin : begin + x.shape[0]] = (silu * up_proj).astype(jnp.bfloat16)
            return unused

        lax.fori_loop(0, pieces, one_piece, 0)

    def share_column(share):
        wanted = lax.broadcasted_iota(jnp.int32, share.shape, 0) == expert
        line = jnp.sum(jnp.where(wanted, share, 0.0), axis=0, keepdims=True)
        down_index = lax.broadcasted_iota(jnp.int32, (rows, rows), 0)
        across_index = lax.broadcasted_iota(jnp.int32, (rows, rows), 1)
        square = jnp.where(down_index == across_index, jnp.broadcast_to(line, (rows, rows)), 0.0)
        return jnp.sum(square, axis=1, keepdims=True)

    tile = width // 4

    def make_parts(slots):
        begin, count = slots[0] * rows, len(slots) * rows
        columns = [share_column(share_ref[...] if slot == 0 else share_slots[slot]) for slot in slots]
        column = jnp.concatenate(columns, axis=0)

        def one_tile(index, unused):
            at = pl.ds(pl.multiple_of(index * tile, tile), tile)
            total = jnp.zeros((count, tile), jnp.float32)
            for piece in range(pieces):
                total = total + lax.dot_general(
                    hidden[piece, begin : begin + count],
                    downs[piece, at, :],
                    (((1,), (1,)), ((), ())),
                    preferred_element_type=jnp.float32,
                )
            parts[begin : begin + count, at] = total.astype(jnp.bfloat16).astype(jnp.float32) * column
            return unused

        lax.fori_loop(0, 4, one_tile, 0)

    def exchange(step):
        ahead, behind = 2 * step - 1, 2 * step
        for which in range(3):
            send(landing(ahead, which), ahead, which, right).wait_recv()
            if step < half - 1:
                send(landing(ahead, which), ahead + 2, which, right).start()
            elif which != 1:
                send(landing(ahead, which), last, which, right).start()
            send(landing(behind, which), behind, which, left).wait_recv()
            if step < half - 1:
                send(landing(behind, which), behind + 2, which, left).start()
            elif which == 1:
                send(landing(behind, which), last, which, left).start()

    def sum_copy(side, step, chunk):
        return pltpu.make_async_remote_copy(
            src_ref=sums_out.at[side, step, chunk],
            dst_ref=sums_in.at[side, step, chunk],
            send_sem=sum_send.at[side, step, chunk],
            recv_sem=sum_recv.at[side, step, chunk],
            device_id={"sp": left if side else right},
            device_id_type=MESH,
        )

    def part_of(side, slot, chunk):
        begin = slot * rows + chunk * half_rows
        return parts[begin : begin + half_rows, side * half_width : (side + 1) * half_width]

    def sum_step(step):
        for chunk in range(2):
            for side in range(2):
                if step < half:
                    slot = 2 * step - 1 + side
                elif step == half:
                    slot = last
                else:
                    slot = 2 * (group - step) - side
                value = part_of(side, slot, chunk)
                if step > 1:
                    sum_copy(side, step - 1, chunk).wait_recv()
                    value = value + sums_in[side, step - 1, chunk].astype(jnp.float32)
                sums_out[side, step, chunk] = value.astype(jnp.bfloat16)
                sum_copy(side, step, chunk).start()

    def pair_hidden(step):
        pair = jnp.concatenate(
            [x_slots[slot, part] for slot in (2 * step - 1, 2 * step) for part in range(2)], axis=0
        )
        make_hidden(pair, (2 * step - 1) * rows)

    exchange(1)
    for load in loads:
        load.wait()
    for copy in near_copies:
        copy.wait_recv()
    pair_hidden(1)
    if half > 2:
        exchange(2)
        pair_hidden(2)
    far_down.wait_recv()
    near_down = weight_send_to(downs.at[2], downs.at[3], 6, near)
    near_down.start()
    near_down.wait_recv()
    make_parts((1, 2))
    for step in range(3, half):
        exchange(step)
        sum_step(step - 2)
        make_parts((2 * step - 3, 2 * step - 2))
        pair_hidden(step)
    if half > 2:
        sum_step(half - 2)
        make_parts((last - 2, last - 1))
    send(landing(last, 0), last, 0, right).wait_recv()
    send(landing(last, 1), last, 1, left).wait_recv()
    send(landing(last, 2), last, 2, right).wait_recv()
    sum_step(half - 1)
    make_hidden(jnp.concatenate([x_slots[last, 0], x_slots[last, 1]], axis=0), last * rows)
    make_parts((last,))
    for step in range(half, group):
        sum_step(step)
        if step == half:
            make_hidden(x_ref[...], 0)
        if step == min(half + 1, last):
            make_parts((0,))
    for chunk in range(2):
        here = slice(chunk * half_rows, (chunk + 1) * half_rows)
        for side in range(2):
            there = slice(side * half_width, (side + 1) * half_width)
            sum_copy(side, last, chunk).wait_recv()
            out_ref[here, there] = (
                carried_ref[here, there].astype(jnp.float32)
                + (part_of(side, 0, chunk) + sums_in[side, last, chunk].astype(jnp.float32))
            ).astype(jnp.bfloat16)
    for slot in range(1, group):
        for which in range(3):
            send(landing(slot, which), slot, which, right).wait_send()
    for step in range(1, group):
        for side in range(2):
            for chunk in range(2):
                sum_copy(side, step, chunk).wait_send()
    for copy in near_copies + [far_down, near_down]:
        copy.wait_send()


def expert_layer(normed, carried, shares, gate, up, down, far_gate, far_up):
    group = lax.axis_size("sp")
    pieces = lax.axis_size("tp")
    rows, width = normed.shape
    units = gate.shape[1]
    vmem = pl.BlockSpec(memory_space=pltpu.VMEM)
    outside = pl.BlockSpec(memory_space=pl.ANY)
    bf16 = jnp.bfloat16
    return pl.pallas_call(
        functools.partial(expert_kernel, group),
        name="experts",
        out_shape=jax.ShapeDtypeStruct((rows, width), bf16),
        in_specs=[vmem] * 3 + [outside] * 5,
        out_specs=vmem,
        scratch_shapes=[
            pltpu.VMEM((group, 2, rows // 2, width), bf16),
            pltpu.VMEM((group,) + shares.shape, jnp.float32),
            pltpu.VMEM((pieces, width, units), bf16),
            pltpu.VMEM((pieces, width, units), bf16),
            pltpu.VMEM((pieces, width, units), bf16),
            pltpu.VMEM((pieces, group * rows, units), bf16),
            pltpu.VMEM((group * rows, width), jnp.float32),
            pltpu.VMEM((2, group, 2, rows // 2, width // 2), bf16),
            pltpu.VMEM((2, group, 2, rows // 2, width // 2), bf16),
            pltpu.SemaphoreType.DMA((3, group)),
            pltpu.SemaphoreType.DMA((3, group)),
            pltpu.SemaphoreType.DMA((2, group, 2)),
            pltpu.SemaphoreType.DMA((2, group, 2)),
            pltpu.SemaphoreType.DMA((5,)),
            pltpu.SemaphoreType.DMA((7,)),
            pltpu.SemaphoreType.DMA((7,)),
        ],
        compiler_params=pltpu.CompilerParams(
            collective_id=1, has_side_effects=True, vmem_limit_bytes=VMEM_BYTES
        ),
    )(normed, carried, shares, gate, up, down, far_gate, far_up)


def nearest_first(position, count, nth):
    order = [
        sorted(range(count), key=lambda other: (abs(other - here), other if 2 * here < count else -other))
        for here in range(count)
    ]
    chosen = jnp.int32(order[0][nth])
    for here in range(1, count):
        chosen = jnp.where(position == here, order[here][nth], chosen)
    return chosen


class WeightFlow:
    def __init__(self, chunks, refs, pieces, send_sems, recv_sems, load_sems):
        gate_ref, up_ref, down_ref = refs
        gates, ups, downs = pieces
        me_tp, tp = lax.axis_index("tp"), lax.axis_size("tp")
        near = me_tp + 1 - 2 * lax.rem(me_tp, 2)
        far = lax.rem(me_tp + tp // 2, tp)
        width = gate_ref.shape[0]
        first, tile = width // 4, width // chunks
        self.used = 0

        def to(target, source, landing):
            index = self.used
            self.used += 1
            return pltpu.make_async_remote_copy(
                src_ref=source,
                dst_ref=landing,
                send_sem=send_sems.at[index],
                recv_sem=recv_sems.at[index],
                device_id={"tp": target},
                device_id_type=MESH,
            )

        cuts = [(0, pl.ds(0, width)), (1, pl.ds(0, first)), (1, pl.ds(first, width - first))]
        cuts += [(2, pl.ds(chunk * tile, tile)) for chunk in range(chunks)]
        self.far = [to(far, refs[kind].at[at], pieces[kind].at[2, at]) for kind, at in cuts]
        self.relays = [to(near, pieces[kind].at[2, at], pieces[kind].at[3, at]) for kind, at in cuts]
        self.near = [to(near, refs[kind], pieces[kind].at[1]) for kind in range(3)]
        self.loads = [
            pltpu.make_async_copy(refs[kind], pieces[kind].at[0], load_sems.at[kind])
            for kind in range(3)
        ]

    def start_far(self, phase):
        if phase == 0:
            for copy in self.far[:2]:
                copy.start()
        else:
            for copy in self.far[2:] + self.near + self.loads:
                copy.start()

    def pass_first(self):
        for far, relay in zip(self.far[:2], self.relays[:2]):
            far.wait_recv()
            relay.start()

    def hidden_ready(self):
        self.far[2].wait_recv()
        self.relays[2].start()
        for copy in self.loads:
            copy.wait()
        for copy in self.near + self.relays[:3]:
            copy.wait_recv()

    def down_ready(self, chunk):
        self.far[3 + chunk].wait_recv()
        self.relays[3 + chunk].start()
        self.relays[3 + chunk].wait_recv()

    def finish(self):
        for copy in self.far + self.relays + self.near:
            copy.wait_send()


def attention_part(
    sides,
    cores,
    start_far,
    q_ref,
    k_ref,
    v_ref,
    lam_ref,
    gain_ref,
    w_out_ref,
    residual_ref,
    norm_gain_ref,
    carried_ref,
    normed_ref,
    q_here,
    kv,
    q_masked,
    peaks,
    totals,
    numerators,
    made,
    came,
    lam_all,
    w_out_here,
    in_send,
    q_recv,
    kv_recv,
    pair_send,
    side_send,
    lam_sems,
    row_send,
    row_recv,
    load_sems,
):
    rows, width = q_ref.shape
    depth = kv.shape[2]
    heads = width // 128
    value_dim = width // heads
    head_dim = value_dim // 2
    half = rows // cores
    exponent_scale = head_dim ** (-0.5) * math.log2(math.e)
    me_sp, me_tp = lax.axis_index("sp"), lax.axis_index("tp")
    tp = lax.axis_size("tp")
    z, y = lax.div(me_sp, sides), lax.rem(me_sp, sides)
    x, c = lax.div(me_tp, cores), lax.rem(me_tp, cores)
    other_y, other_c = 1 - y, 1 - c

    def device(at_z, at_y, at_x, at_c):
        return {"sp": at_z * sides + at_y, "tp": at_x * cores + at_c}

    lam_row = lax.broadcasted_iota(jnp.int32, lam_all.shape[1:], 0)
    lam_block = jnp.zeros(lam_all.shape[1:], jnp.float32)
    for head in range(heads):
        lam_block = jnp.where(lam_row == head, lam_ref[head], lam_block)
    lam_all[c] = lam_block

    barrier = pltpu.get_barrier_semaphore()
    plane = depth * tp
    spot = z * tp + me_tp
    for step in range(1, plane):
        peer = lax.rem(spot + step, plane)
        pl.semaphore_signal(
            barrier,
            inc=1,
            device_id={"sp": lax.div(peer, tp) * sides + y, "tp": lax.rem(peer, tp)},
            device_id_type=MESH,
        )
    pl.semaphore_signal(barrier, inc=1, device_id=device(z, other_y, x, c), device_id_type=MESH)
    pl.semaphore_wait(barrier, plane)

    def remote(source, landing, send_sem, recv_sem, target):
        return pltpu.make_async_remote_copy(
            src_ref=source,
            dst_ref=landing,
            send_sem=send_sem,
            recv_sem=recv_sem,
            device_id=target,
            device_id_type=MESH,
        )

    def deliver(source, landing, send_sem, recv_sem, target, stays):
        @pl.when(stays)
        def _():
            pltpu.make_async_copy(source, landing, recv_sem).start()

        @pl.when(jnp.logical_not(stays))
        def _():
            remote(source, landing, send_sem, recv_sem, target).start()

    def left(source, landing, send_sem, recv_sem, target, stays):
        @pl.when(jnp.logical_not(stays))
        def _():
            remote(source, landing, send_sem, recv_sem, target).wait_send()

    inputs = []
    for head in range(heads):
        columns = slice(head * value_dim, (head + 1) * value_dim)
        to_z = c * heads + head
        for core in range(cores):
            inputs.append(
                (
                    q_ref.at[core * half : (core + 1) * half, columns],
                    q_here.at[z],
                    in_send.at[head, core],
                    q_recv.at[z],
                    device(to_z, y, x, core),
                    jnp.logical_and(to_z == z, c == core),
                )
            )
    for head in range(heads):
        columns = slice(head * value_dim, (head + 1) * value_dim)
        to_z = c * heads + head
        for core, source in ((0, k_ref), (1, v_ref)):
            inputs.append(
                (
                    source.at[:, columns],
                    kv.at[core, y, z],
                    in_send.at[head, cores + core],
                    kv_recv.at[core, y, z],
                    device(to_z, y, x, core),
                    jnp.logical_and(to_z == z, c == core),
                )
            )
    lam_copy = remote(lam_all.at[c], lam_all.at[c], lam_sems.at[0], lam_sems.at[1], device(z, y, x, other_c))
    for item in inputs:
        deliver(*item)
    lam_copy.start()
    start_far(0)
    load_w_out = pltpu.make_async_copy(w_out_ref, w_out_here, load_sems.at[0])
    load_w_out.start()

    peaks[...] = jnp.full(peaks.shape, FLOOR_SCORE, jnp.float32)
    totals[...] = jnp.zeros(totals.shape, jnp.float32)
    numerators[...] = jnp.zeros(numerators.shape, jnp.float32)

    def block_wait(tensor, side, at):
        slot = kv.at[tensor, side, at]
        remote(
            slot, slot, pair_send.at[0, 0], kv_recv.at[tensor, side, at], device(z, other_y, x, c)
        ).wait_recv()

    def to_pair(side, at):
        slot = kv.at[c, side, at]
        return remote(
            slot, slot, pair_send.at[side, at], kv_recv.at[c, side, at], device(z, y, x, other_c)
        )

    def to_side(at):
        slot = kv.at[c, y, at]
        return remote(
            slot, slot, side_send.at[at], kv_recv.at[c, y, at], device(z, other_y, x, c)
        )

    def take_own(at):
        block_wait(c, y, at)
        to_side(at).start()
        to_pair(y, at).start()

    def take_side(at):
        block_wait(c, other_y, at)
        to_pair(other_y, at).start()

    def absorb(places, part):
        if part == 0:
            for side, at in places:
                block_wait(other_c, side, at)
        key_block = jnp.concatenate([kv[0, side, at] for side, at in places], axis=0)
        value_block = jnp.concatenate([kv[1, side, at] for side, at in places], axis=0)
        count = len(places) * rows
        with_ones = jnp.concatenate([value_block, jnp.ones((count, 128), jnp.bfloat16)], axis=1)

        def scores_of(begin):
            return lax.dot_general(
                q_masked[part, begin : begin + half],
                key_block,
                (((1,), (1,)), ((), ())),
                preferred_element_type=jnp.float32,
            )

        coming = scores_of(0)
        for begin in range(0, depth * half, half):
            here = slice(begin, begin + half)
            scores = coming
            if begin + half < depth * half:
                coming = scores_of(begin + half)
            old_peak = peaks[part, here]
            row_peak = jnp.broadcast_to(jnp.max(scores, axis=1, keepdims=True), (half, 128))
            new_peak = jnp.maximum(old_peak, row_peak)
            level = jnp.concatenate([new_peak] * (count // 128), axis=1)
            weights = jnp.exp2((scores - level) * exponent_scale)
            shrink = jnp.exp2((old_peak - new_peak) * exponent_scale)
            product = jnp.dot(
                weights.astype(jnp.bfloat16), with_ones, preferred_element_type=jnp.float32
            )
            numerators[part, here] = numerators[part, here] * shrink + product[:, :value_dim]
            totals[part, here] = totals[part, here] * shrink + product[:, value_dim:]
            peaks[part, here] = new_peak

    take_own(z)
    take_side(z)
    lane = lax.broadcasted_iota(jnp.int32, (half, value_dim), 1)
    for at in range(depth):
        remote(
            q_here.at[at], q_here.at[at], pair_send.at[0, 0], q_recv.at[at], device(z, other_y, x, c)
        ).wait_recv()
        both = q_here[at]
        here = slice(at * half, (at + 1) * half)
        q_masked[0, here] = jnp.where(lane < head_dim, both, jnp.zeros_like(both))
        q_masked[1, here] = jnp.where(lane >= head_dim, both, jnp.zeros_like(both))

    def nth(index):
        chosen = nearest_first(z, depth, 0)
        for place in range(1, depth):
            chosen = jnp.where(index == place, nearest_first(z, depth, place), chosen)
        return chosen

    absorb([(y, z)], 0)
    take_own(nth(1))
    absorb([(y, z)], 1)

    def one_block(index, unused):
        at, before = nth(index), nth(index - 1)
        absorb([(y, at), (other_y, before)], 0)

        @pl.when(index < depth - 1)
        def _():
            take_own(nth(index + 1))

        take_side(at)
        absorb([(y, at), (other_y, before)], 1)
        return unused

    lax.fori_loop(1, depth, one_block, 0)
    last = nth(depth - 1)
    absorb([(other_y, last)], 0)
    absorb([(other_y, last)], 1)

    lam_copy.wait_recv()
    lam_here = lam_all[lax.div(z, heads)]
    lam = jnp.sum(jnp.where(lam_row == lax.rem(z, heads), lam_here, 0.0), axis=0, keepdims=True)
    gain = gain_ref[...] * OUT_SCALE
    dev_rows = residual_ref.shape[0]
    my_head = x * depth + z

    def row_item(at, part):
        return (
            made.at[at, part * dev_rows : (part + 1) * dev_rows],
            came.at[my_head],
            row_send.at[at, part],
            row_recv.at[my_head],
            device(at, y, c, part),
            jnp.logical_and(at == z, jnp.logical_and(x == c, c == part)),
        )

    for place in reversed(range(depth)):
        at = nearest_first(z, depth, place)
        here = pl.ds(pl.multiple_of(at * half, half), half)
        first = numerators[0, here] / totals[0, here][:, :1]
        second = numerators[1, here] / totals[1, here][:, :1]
        combined = first - lam * second
        mean_square = jnp.mean(combined * combined, axis=1, keepdims=True)
        made[at] = (combined * lax.rsqrt(mean_square + EPSILON) * gain).astype(jnp.bfloat16)
        for part in range(half // dev_rows):
            deliver(*row_item(at, part))
    start_far(1)
    load_w_out.wait()
    for head in range(came.shape[0]):
        remote(
            came.at[head], came.at[head], pair_send.at[0, 0], row_recv.at[head], device(z, other_y, x, c)
        ).wait_recv()
    attended = jnp.concatenate([came[head] for head in range(came.shape[0])], axis=1)
    mixed = jnp.dot(attended, w_out_here[...], preferred_element_type=jnp.float32).astype(
        jnp.bfloat16
    )
    carried = (residual_ref[...].astype(jnp.float32) + mixed.astype(jnp.float32)).astype(
        jnp.bfloat16
    )
    carried_ref[...] = carried
    wide = carried.astype(jnp.float32)
    spread = jnp.mean(wide * wide, axis=1, keepdims=True)
    normed_ref[...] = (wide * lax.rsqrt(spread + EPSILON) * norm_gain_ref[...]).astype(
        jnp.bfloat16
    )

    def finish():
        for item in inputs:
            left(*item)
        lam_copy.wait_send()
        for at in range(depth):
            to_side(at).wait_send()
            to_pair(0, at).wait_send()
            to_pair(1, at).wait_send()
            for part in range(half // dev_rows):
                left(*row_item(at, part))

    return finish


def expert_part(
    sides,
    weights,
    x_ref,
    carried_ref,
    share_ref,
    out_ref,
    x_all,
    share_all,
    selections,
    columns,
    takes,
    picked,
    packed_out,
    gates,
    ups,
    downs,
    hidden,
    results_out,
    results_in,
    results_own,
    parts,
    sums_in,
    sums_out,
    out_here,
    out_sems,
    x_send,
    x_recv,
    share_send,
    share_recv,
    pack_send,
    pack_recv,
    result_send,
    result_recv,
    sum_send,
    sum_recv,
):
    rows, width = x_ref.shape
    depth = x_all.shape[0]
    capacity = rows // 2
    pieces = gates.shape[0]
    chunks = x_recv.shape[1]
    tile = width // chunks
    splits = sum_send.shape[1] // chunks
    fine_tile = tile // splits
    me_sp, me_tp = lax.axis_index("sp"), lax.axis_index("tp")
    z, y = lax.div(me_sp, sides), lax.rem(me_sp, sides)
    partner = z * sides + 1 - y
    has_below, has_above = z > 0, z < depth - 1
    middle = jnp.logical_and(has_below, has_above)
    blocks = [nearest_first(z, depth, place) for place in range(depth)]

    def remote(source, landing, send_sem, recv_sem, target):
        return pltpu.make_async_remote_copy(
            src_ref=source,
            dst_ref=landing,
            send_sem=send_sem,
            recv_sem=recv_sem,
            device_id=target,
            device_id_type=MESH,
        )

    below, above = {"sp": me_sp - sides}, {"sp": me_sp + sides}

    def cut(chunk):
        return pl.ds(chunk * tile, tile)

    def x_copy(source, block, chunk, downward):
        return remote(
            source.at[:, cut(chunk)],
            x_all.at[block, :, cut(chunk)],
            x_send.at[downward, block, chunk],
            x_recv.at[block, chunk],
            below if downward else above,
        )

    def share_copy(source, block, downward):
        return remote(
            source,
            share_all.at[block],
            share_send.at[downward, block],
            share_recv.at[block],
            below if downward else above,
        )

    for downward, exists in ((0, has_above), (1, has_below)):

        @pl.when(exists)
        def _():
            share_copy(share_ref, z, downward).start()
            for chunk in range(chunks):
                x_copy(x_ref, z, chunk, downward).start()

    def to_far(index, source, landing):
        return remote(source, landing, weight_send.at[index], weight_recv.at[index], {"tp": far})

    def to_near(index, source, landing):
        return remote(source, landing, weight_send.at[index], weight_recv.at[index], {"tp": near})

    def select(step, share):
        named = (share > 0.0).astype(jnp.float32)
        earlier = lax.broadcasted_iota(jnp.int32, (rows, rows), 0) < lax.broadcasted_iota(
            jnp.int32, (rows, rows), 1
        )
        rank = jnp.dot(
            named.astype(jnp.bfloat16),
            earlier.astype(jnp.float32).astype(jnp.bfloat16),
            preferred_element_type=jnp.float32,
        )
        expert_row = lax.broadcasted_iota(jnp.int32, share.shape, 0)
        slot = lax.broadcasted_iota(jnp.int32, (capacity, rows), 0).astype(jnp.float32)
        diagonal = lax.broadcasted_iota(jnp.int32, (rows, rows), 0) == lax.broadcasted_iota(
            jnp.int32, (rows, rows), 1
        )
        found = []
        for side, expert in enumerate((partner, me_sp)):

            def line(table):
                return jnp.sum(jnp.where(expert_row == expert, table, 0.0), axis=0, keepdims=True)

            taken = jnp.where(jnp.logical_and(slot == line(rank), line(named) > 0.0), 1.0, 0.0)
            found.append(taken)
            selections[step, side] = taken.T.astype(jnp.bfloat16)
            square = jnp.where(diagonal, jnp.broadcast_to(line(share), (rows, rows)), 0.0)
            columns[step, side] = jnp.broadcast_to(
                jnp.sum(square, axis=1, keepdims=True), (rows, 128)
            )
        return jnp.concatenate(found, axis=0).astype(jnp.bfloat16)

    def pack_copy(step, chunk):
        return remote(
            packed_out.at[step, :, cut(chunk)],
            picked.at[pl.ds(step * rows, capacity), cut(chunk)],
            pack_send.at[step, chunk],
            pack_recv.at[step, chunk],
            {"sp": partner},
        )

    def pack(step, chunk):
        block = x_ref[:, cut(chunk)] if step == 0 else x_all[blocks[step], :, cut(chunk)]
        compact = jnp.dot(takes[step], block, preferred_element_type=jnp.float32).astype(jnp.bfloat16)
        packed_out[step, :, cut(chunk)] = compact[:capacity]
        picked[step * rows + capacity : (step + 1) * rows, cut(chunk)] = compact[capacity:]
        pack_copy(step, chunk).start()

    def forward(step, chunk):
        block = blocks[step]
        go_up = jnp.logical_and(block < z, has_above)
        go_down = jnp.logical_and(block > z, has_below)
        if chunk == 0:
            share_copy(share_all.at[block], block, 0).wait_recv()
        x_copy(x_all.at[block], block, chunk, 0).wait_recv()
        for downward, goes in ((0, go_up), (1, go_down)):

            @pl.when(goes)
            def _():
                if chunk == 0:
                    share_copy(share_all.at[block], block, downward).start()
                x_copy(x_all.at[block], block, chunk, downward).start()

    def choose(step):
        takes[step] = select(step, share_ref[...] if step == 0 else share_all[blocks[step]])

    def pack_all(step):
        choose(step)
        for chunk in range(chunks):
            pack(step, chunk)

    def bring(step, chunk):
        forward(step, chunk)
        if chunk == 0:
            choose(step)
        pack(step, chunk)

    def make_hidden(first, last, piece):
        here = slice(first * rows, last * rows)
        x = picked[here]
        gate_proj = jnp.dot(x, gates[piece], preferred_element_type=jnp.float32)
        up_proj = jnp.dot(x, ups[piece], preferred_element_type=jnp.float32)
        silu = gate_proj / (1.0 + jnp.exp(-gate_proj))
        hidden[piece, here] = (silu * up_proj).astype(jnp.bfloat16)

    def result_copy(step, chunk):
        return remote(
            results_out.at[step, :, cut(chunk)],
            results_in.at[step, :, cut(chunk)],
            result_send.at[step, chunk],
            result_recv.at[step, chunk],
            {"sp": partner},
        )

    def make_results(first, last, chunk):
        total = jnp.zeros(((last - first) * rows, tile), jnp.float32)
        for piece in range(pieces):
            total = total + lax.dot_general(
                hidden[piece, first * rows : last * rows],
                downs[piece, cut(chunk)],
                (((1,), (1,)), ((), ())),
                preferred_element_type=jnp.float32,
            )
        total = total.astype(jnp.bfloat16)
        for step in range(first, last):
            at = (step - first) * rows
            results_out[step, :, cut(chunk)] = total[at : at + capacity]
            results_own[step, :, cut(chunk)] = total[at + capacity : at + rows]
            result_copy(step, chunk).start()

    def spread(step, chunk):
        result_copy(step, chunk).wait_recv()
        theirs = jnp.dot(
            selections[step, 0], results_in[step, :, cut(chunk)], preferred_element_type=jnp.float32
        )
        ours = jnp.dot(
            selections[step, 1], results_own[step, :, cut(chunk)], preferred_element_type=jnp.float32
        )
        parts[step, :, cut(chunk)] = theirs * columns[step, 0][:, :1] + ours * columns[step, 1][:, :1]

    def fine_cut(chunk):
        return pl.ds(chunk * fine_tile, fine_tile)

    def sum_copy(step, chunk, downward):
        block = blocks[step]
        return remote(
            sums_out.at[step, :, fine_cut(chunk)],
            sums_in.at[downward, block, :, fine_cut(chunk)],
            sum_send.at[step, chunk],
            sum_recv.at[downward, block, chunk],
            below if downward else above,
        )

    def pass_sum(step, chunk, has_outer):
        pass_fine(step, range(chunk * splits, (chunk + 1) * splits), has_outer)

    def pass_fine(step, fines, has_outer):
        block = blocks[step]
        for downward, goes in ((0, block > z), (1, block < z)):

            @pl.when(goes)
            def _():
                for fine in fines:
                    value = parts[step, :, fine_cut(fine)]
                    if has_outer:
                        sum_copy(step, fine, downward).wait_recv()
                        value = value + sums_in[downward, block, :, fine_cut(fine)].astype(jnp.float32)
                    sums_out[step, :, fine_cut(fine)] = value.astype(jnp.bfloat16)
                    sum_copy(step, fine, downward).start()

    def at_end(action):
        pl.when(jnp.logical_not(middle))(action)

    def at_middle(action):
        pl.when(middle)(action)

    def packed(step):
        for chunk in range(chunks):
            pack_copy(step, chunk).wait_recv()

    def all_hidden(step):
        for piece in range(pieces):
            make_hidden(step, step + 1, piece)

    def settle(step, chunk):
        spread(step, chunk)
        at_end(functools.partial(pass_sum, step, chunk, False))

    def second(chunk):
        at_end(functools.partial(bring, 2, chunk))
        at_middle(functools.partial(bring, 3, chunk))

    def third(chunk):
        at_end(functools.partial(bring, 3, chunk))

    pack_all(0)
    weights.pass_first()
    for chunk in range(chunks):
        bring(1, chunk)
        at_middle(functools.partial(forward, 2, chunk))
    at_middle(functools.partial(pack_all, 2))
    weights.hidden_ready()
    second(0)
    packed(1)
    all_hidden(1)
    second(1)
    weights.down_ready(0)
    make_results(1, 2, 0)
    second(2)
    weights.down_ready(1)
    make_results(1, 2, 1)
    second(3)
    settle(1, 0)
    packed(2)
    all_hidden(2)
    make_results(2, 3, 0)
    make_results(2, 3, 1)
    third(0)
    settle(1, 1)
    third(1)
    weights.down_ready(2)
    make_results(1, 3, 2)
    third(2)
    settle(2, 0)
    settle(2, 1)
    settle(1, 2)
    third(3)
    weights.down_ready(3)
    make_results(1, 3, 3)
    settle(2, 2)
    packed(3)
    all_hidden(3)
    for chunk in range(chunks):
        make_results(3, 4, chunk)
    settle(1, 3)
    settle(2, 3)
    packed(0)
    all_hidden(0)
    for chunk in range(chunks):
        make_results(0, 1, chunk)
    for chunk in range(chunks):
        at_middle(functools.partial(pass_sum, 2, chunk, True))
    for chunk in range(chunks):
        spread(3, chunk)
        at_end(functools.partial(pass_sum, 3, chunk, False))

    @at_middle
    def _():
        lag, fines = 3, chunks * splits
        for fine in range(fines + lag):
            if fine < fines:
                pass_fine(3, (fine,), True)
            if fine >= lag:
                pass_fine(1, (fine - lag,), True)

    stores = []
    for chunk in range(chunks):
        spread(0, chunk)
    for chunk in range(chunks):
        here = cut(chunk)

        def arrived(downward):
            for fine in range(chunk * splits, (chunk + 1) * splits):
                there = fine_cut(fine)
                landing = sums_in.at[downward, z, :, there]
                remote(
                    landing, landing, sum_send.at[0, fine], sum_recv.at[downward, z, fine], above
                ).wait_recv()
                parts[0, :, there] = parts[0, :, there] + sums_in[downward, z, :, there].astype(
                    jnp.float32
                )

        pl.when(has_below)(functools.partial(arrived, 0))
        pl.when(has_above)(functools.partial(arrived, 1))
        out_here[:, here] = (carried_ref[:, here].astype(jnp.float32) + parts[0, :, here]).astype(
            jnp.bfloat16
        )
        stores.append(pltpu.make_async_copy(out_here.at[:, here], out_ref.at[:, here], out_sems.at[chunk]))
        stores[-1].start()

    for downward, exists in ((0, has_above), (1, has_below)):

        @pl.when(exists)
        def _():
            share_copy(share_ref, z, downward).wait_send()
            for chunk in range(chunks):
                x_copy(x_ref, z, chunk, downward).wait_send()

    for step in range(1, depth):
        block = blocks[step]
        for downward, goes in (
            (0, jnp.logical_and(block < z, has_above)),
            (1, jnp.logical_and(block > z, has_below)),
        ):

            @pl.when(goes)
            def _():
                share_copy(share_all.at[block], block, downward).wait_send()
                for chunk in range(chunks):
                    x_copy(x_all.at[block], block, chunk, downward).wait_send()

    for step in range(depth):
        for chunk in range(chunks):
            pack_copy(step, chunk).wait_send()
            result_copy(step, chunk).wait_send()
        if step:
            for chunk in range(chunks * splits):
                sum_copy(step, chunk, 0).wait_send()

    return stores


def layer_kernel(sides, cores, chunks, *refs):
    inputs, rest = refs[:8], refs[8:]
    ids_ref, shares_ref, gate_ref, up_ref, down_ref, out_ref = rest[:6]
    carried, normed, share_here = rest[6:9]
    attention_scratch, rest = rest[9:28], rest[28:]
    dev_rows, routes = ids_ref.shape
    lane = lax.broadcasted_iota(jnp.int32, (dev_rows, 128), 1)
    table = jnp.zeros((dev_rows, 128), jnp.float32)
    for route in range(routes):
        hit = ids_ref[:, route : route + 1] == lane
        table = table + jnp.where(hit, shares_ref[:, route : route + 1], 0.0)
    share_here[...] = table.T[: share_here.shape[0]]
    expert_scratch, (weight_send, weight_recv, weight_loads) = rest[:-3], rest[-3:]
    weights = WeightFlow(
        chunks,
        (gate_ref, up_ref, down_ref),
        expert_scratch[7:10],
        weight_send,
        weight_recv,
        weight_loads,
    )
    finish = attention_part(
        sides, cores, weights.start_far, *inputs, carried, normed, *attention_scratch
    )
    stores = expert_part(sides, weights, normed, carried, share_here, out_ref, *expert_scratch)
    finish()
    weights.finish()
    for copy in stores:
        copy.wait()


def whole_layer(
    queries,
    keys,
    values,
    lambdas,
    head_gain,
    w_out,
    residual_in,
    norm_gain,
    route_ids,
    route_weight,
    gate,
    up,
    down,
):
    tp = lax.axis_size("tp")
    sides, cores, chunks = 2, 2, 4
    experts = lax.axis_size("sp")
    depth = experts // sides
    rows, width = queries.shape
    dev_rows, model_width = residual_in.shape
    units = gate.shape[1]
    value_dim = 128
    heads_all = (width // value_dim) * tp
    half = rows // cores
    capacity = dev_rows // 2
    vmem = pl.BlockSpec(memory_space=pltpu.VMEM)
    smem = pl.BlockSpec(memory_space=pltpu.SMEM)
    outside = pl.BlockSpec(memory_space=pl.ANY)
    bf16, f32 = jnp.bfloat16, jnp.float32
    dma = pltpu.SemaphoreType.DMA
    attention_scratch = [
        pltpu.VMEM((depth, half, value_dim), bf16),
        pltpu.VMEM((2, sides, depth, rows, value_dim), bf16),
        pltpu.VMEM((2, depth * half, value_dim), bf16),
        pltpu.VMEM((2, depth * half, 128), f32),
        pltpu.VMEM((2, depth * half, 128), f32),
        pltpu.VMEM((2, depth * half, value_dim), f32),
        pltpu.VMEM((depth, half, value_dim), bf16),
        pltpu.VMEM((heads_all, dev_rows, value_dim), bf16),
        pltpu.VMEM((cores, 8, 128), f32),
        pltpu.VMEM(w_out.shape, bf16),
        dma((width // value_dim, 2 * cores)),
        dma((depth,)),
        dma((2, sides, depth)),
        dma((sides, depth)),
        dma((depth,)),
        dma((2,)),
        dma((depth, half // dev_rows)),
        dma((heads_all,)),
        dma((1,)),
    ]
    expert_scratch = [
        pltpu.VMEM((depth, dev_rows, model_width), bf16),
        pltpu.VMEM((depth, experts, dev_rows), f32),
        pltpu.VMEM((depth, 2, dev_rows, capacity), bf16),
        pltpu.VMEM((depth, 2, dev_rows, 128), f32),
        pltpu.VMEM((depth, dev_rows, dev_rows), bf16),
        pltpu.VMEM((depth * dev_rows, model_width), bf16),
        pltpu.VMEM((depth, capacity, model_width), bf16),
        pltpu.VMEM((tp, model_width, units), bf16),
        pltpu.VMEM((tp, model_width, units), bf16),
        pltpu.VMEM((tp, model_width, units), bf16),
        pltpu.VMEM((tp, depth * dev_rows, units), bf16),
        pltpu.VMEM((depth, capacity, model_width), bf16),
        pltpu.VMEM((depth, capacity, model_width), bf16),
        pltpu.VMEM((depth, capacity, model_width), bf16),
        pltpu.VMEM((depth, dev_rows, model_width), f32),
        pltpu.VMEM((2, depth, dev_rows, model_width), bf16),
        pltpu.VMEM((depth, dev_rows, model_width), bf16),
        pltpu.VMEM((dev_rows, model_width), bf16),
        dma((chunks,)),
        dma((2, depth, chunks)),
        dma((depth, chunks)),
        dma((2, depth)),
        dma((depth,)),
        dma((depth, chunks)),
        dma((depth, chunks)),
        dma((depth, chunks)),
        dma((depth, chunks)),
        dma((depth, 2 * chunks)),
        dma((2, depth, 2 * chunks)),
    ]
    weight_copies = 2 * (chunks + 3) + 3
    return pl.pallas_call(
        functools.partial(layer_kernel, sides, cores, chunks),
        name="layer",
        out_shape=jax.ShapeDtypeStruct((dev_rows, model_width), bf16),
        in_specs=[vmem, vmem, vmem, smem, vmem, outside] + [vmem] * 4 + [outside] * 3,
        out_specs=outside,
        scratch_shapes=[
            pltpu.VMEM((dev_rows, model_width), bf16),
            pltpu.VMEM((dev_rows, model_width), bf16),
            pltpu.VMEM((experts, dev_rows), f32),
        ]
        + attention_scratch
        + expert_scratch
        + [dma((weight_copies,)), dma((weight_copies,)), dma((3,))],
        compiler_params=pltpu.CompilerParams(
            collective_id=2, has_side_effects=True, vmem_limit_bytes=VMEM_BYTES
        ),
    )(
        queries,
        keys,
        values,
        lambdas,
        head_gain.reshape(1, -1),
        w_out,
        residual_in,
        norm_gain.reshape(1, -1),
        route_ids,
        route_weight,
        gate,
        up,
        down,
    )


def weight_pieces(weights):
    pieces = [weights]
    for bit in reversed(range(lax.axis_size("tp").bit_length() - 1)):
        pieces = pieces + [
            tuple(swapped(array, "tp", bit) for array in piece) for piece in pieces
        ]
    return pieces


def local(
    queries,
    keys,
    values,
    lambdas,
    head_gain,
    w_out,
    residual_in,
    norm_gain,
    route_ids,
    route_weight,
    w_gate,
    w_up,
    w_down,
):
    sp_size, tp_size = lax.axis_size("sp"), lax.axis_size("tp")
    whole_heads = lambdas.shape[0] * 128 == queries.shape[1]
    square = queries.shape[0] == 2 * 2 * residual_in.shape[0]
    columns_fit = sp_size == 8 and tp_size == 4 and lambdas.shape[0] == 2 and whole_heads and square
    if columns_fit and w_gate.shape[0] == 1:
        tensors = (queries, keys, values, lambdas, head_gain, w_out, residual_in, norm_gain)
        return whole_layer(*tensors, route_ids, route_weight, w_gate[0], w_up[0], w_down[0])
    carried, normed, far_gate, far_up = attend(
        queries,
        keys,
        values,
        lambdas,
        head_gain,
        w_out,
        residual_in,
        norm_gain,
        w_gate.reshape(-1, w_gate.shape[-1]),
        w_up.reshape(-1, w_up.shape[-1]),
    )
    if w_gate.shape[0] == 1 and 4 <= sp_size <= 8 and tp_size == 4:
        named = lax.broadcasted_iota(jnp.int32, (sp_size, residual_in.shape[0], 2), 0)
        shares = jnp.sum(jnp.where(named == route_ids[None], route_weight[None], 0.0), axis=2)
        return expert_layer(
            normed, carried, shares, w_gate[0], w_up[0], w_down[0], far_gate, far_up
        )
    pieces = weight_pieces((w_gate, w_up, w_down))
    carried_wide = carried.astype(jnp.float32)
    dev_rows = residual_in.shape[0]
    model_width = normed.shape[1]
    experts_here = w_gate.shape[0]
    expert_count = experts_here * lax.axis_size("sp")
    capacity = max(2, 4 * dev_rows // expert_count)
    flat_ids = route_ids.reshape(-1)
    targets = flat_ids * capacity + slot_numbers(flat_ids)
    slot_ids = lax.broadcasted_iota(jnp.int32, (expert_count * capacity, dev_rows, 2), 0)
    placement_matrix = jnp.sum(
        (targets.reshape(1, dev_rows, 2) == slot_ids).astype(jnp.int32), axis=2
    ).astype(jnp.bfloat16)
    outgoing = jnp.dot(placement_matrix, normed, preferred_element_type=jnp.float32).astype(
        jnp.bfloat16
    )
    outgoing = outgoing.reshape(lax.axis_size("sp"), experts_here, capacity, model_width)
    arrived = lax.all_to_all(outgoing, "sp", split_axis=0, concat_axis=0, tiled=True)
    summed = 0.0
    for gate_piece, up_piece, down_piece in pieces:
        gate_proj = jnp.einsum("secd,edf->secf", arrived, gate_piece, preferred_element_type=jnp.float32)
        up_proj = jnp.einsum("secd,edf->secf", arrived, up_piece, preferred_element_type=jnp.float32)
        hidden = (jax.nn.silu(gate_proj) * up_proj).astype(jnp.bfloat16)
        summed = summed + jnp.einsum(
            "secf,edf->secd", hidden, down_piece, preferred_element_type=jnp.float32
        )
    returned = send_back(summed.astype(jnp.bfloat16))
    flat_back = returned.reshape(expert_count * capacity, model_width)
    picked = (
        jnp.take(flat_back, targets, axis=0).astype(jnp.float32).reshape(dev_rows, 2, model_width)
    )
    layer_out = carried_wide + jnp.sum(route_weight[..., None] * picked, axis=1)
    return layer_out.astype(jnp.bfloat16)


def solution(mesh):
    placed = (
        P("sp", "tp"),
        P("sp", "tp"),
        P("sp", "tp"),
        P("tp"),
        P(),
        P(),
        P(("sp", "tp"), None),
        P(),
        P(("sp", "tp"), None),
        P(("sp", "tp"), None),
        P("sp", None, "tp"),
        P("sp", None, "tp"),
        P("sp", None, "tp"),
    )
    return jax.shard_map(
        local, mesh=mesh, in_specs=placed, out_specs=P(("sp", "tp"), None), check_vma=False
    )
```

```python
import functools
import math

import jax
import jax.numpy as jnp
from jax import lax
from jax.experimental import pallas as pl
from jax.experimental.pallas import tpu as pltpu
from jax.sharding import PartitionSpec as P

EPSILON = 1e-06
OUT_SCALE = 0.8
FLOOR_SCORE = -1e30


def swapped(value, axis, distance):
    mask = 2**distance
    pairs = [(source, source ^ mask) for source in range(lax.axis_size(axis))]
    return lax.ppermute(value, axis, pairs)


def slot_numbers(flat_ids):
    count_ids = flat_ids.shape[0]
    positions = lax.broadcasted_iota(jnp.int32, (count_ids, count_ids), 0)
    earlier = lax.broadcasted_iota(jnp.int32, (count_ids, count_ids), 1) < positions
    matches = (flat_ids[:, None] == flat_ids[None, :]) & earlier
    return jnp.sum(matches.astype(jnp.int32), axis=1)


def send_back(results):
    return lax.all_to_all(results, "sp", split_axis=0, concat_axis=0, tiled=True)

MESH = pl.DeviceIdType.MESH
VMEM_BYTES = 60 * 1024 * 1024


def ring_neighbours(group):
    me = lax.axis_index("sp")
    spot = lax.rem(me, group)
    base = me - spot
    even = lax.rem(spot, 2) == 0
    up = jnp.where(even, jnp.where(spot == group - 2, group - 1, spot + 2), jnp.where(spot == 1, 0, spot - 2))
    down = jnp.where(even, jnp.where(spot == 0, 1, spot - 2), jnp.where(spot == group - 1, group - 2, spot + 2))
    return base + up, base + down


def attention_kernel(
    group,
    tp,
    q_ref,
    k_ref,
    v_ref,
    lam_ref,
    gain_ref,
    w_out_ref,
    residual_ref,
    norm_gain_ref,
    gate_ref,
    up_ref,
    carried_ref,
    normed_ref,
    far_gate_ref,
    far_up_ref,
    k_slots,
    v_slots,
    q_masked,
    peaks,
    totals,
    numerators,
    made,
    came,
    w_out_here,
    send_sems,
    recv_sems,
    row_send,
    row_recv,
    load_sems,
    far_send,
    far_recv,
):
    rows = q_ref.shape[0]
    heads = lam_ref.shape[0]
    value_dim = v_ref.shape[1] // heads
    head_dim = value_dim // 2
    exponent_scale = head_dim ** (-0.5) * math.log2(math.e)
    right, left = ring_neighbours(group)
    me_tp = lax.axis_index("tp")

    barrier = pltpu.get_barrier_semaphore()
    for neighbour in (right, left):
        pl.semaphore_signal(barrier, inc=1, device_id={"sp": neighbour}, device_id_type=MESH)
    for step in range(1, tp):
        pl.semaphore_signal(
            barrier, inc=1, device_id={"tp": lax.rem(me_tp + step, tp)}, device_id_type=MESH
        )
    pl.semaphore_wait(barrier, 2 + tp - 1)

    def send(source, slots, which, slot, target):
        return pltpu.make_async_remote_copy(
            src_ref=source,
            dst_ref=slots.at[slot],
            send_sem=send_sems.at[which, slot],
            recv_sem=recv_sems.at[which, slot],
            device_id={"sp": target},
            device_id_type=MESH,
        )

    last = group - 1
    if group > 2:
        for slot, target in ((1, right), (2, left)):
            send(k_ref, k_slots, 0, slot, target).start()
            send(v_ref, v_slots, 1, slot, target).start()
    elif group == 2:
        send(k_ref, k_slots, 0, 1, right).start()
        send(v_ref, v_slots, 1, 1, left).start()
    own_loads = (
        pltpu.make_async_copy(k_ref, k_slots.at[0], load_sems.at[0]),
        pltpu.make_async_copy(v_ref, v_slots.at[0], load_sems.at[1]),
    )
    for load in own_loads:
        load.start()
    load_w_out = pltpu.make_async_copy(w_out_ref, w_out_here, load_sems.at[2])
    load_w_out.start()

    far_copies = [
        pltpu.make_async_remote_copy(
            src_ref=source,
            dst_ref=landing,
            send_sem=far_send.at[index],
            recv_sem=far_recv.at[index],
            device_id={"tp": lax.rem(me_tp + tp // 2, tp)},
            device_id_type=MESH,
        )
        for index, (source, landing) in enumerate(((gate_ref, far_gate_ref), (up_ref, far_up_ref)))
    ]
    for copy in far_copies:
        copy.start()

    lane = lax.broadcasted_iota(jnp.int32, (rows, value_dim), 1)
    for head in range(heads):
        both = q_ref[:, head * value_dim : (head + 1) * value_dim]
        q_masked[2 * head] = jnp.where(lane < head_dim, both, jnp.zeros_like(both))
        q_masked[2 * head + 1] = jnp.where(lane >= head_dim, both, jnp.zeros_like(both))
    peaks[...] = jnp.full(peaks.shape, FLOOR_SCORE, jnp.float32)
    totals[...] = jnp.zeros(totals.shape, jnp.float32)
    numerators[...] = jnp.zeros(numerators.shape, jnp.float32)
    for load in own_loads:
        load.wait()

    chunk = min(rows, 256)

    def absorb(slot, count):
        keys_here = count * k_slots.shape[1]
        for head in range(heads):
            columns = slice(head * value_dim, (head + 1) * value_dim)
            key_block = k_slots[pl.ds(slot, count), :, columns].reshape(keys_here, value_dim)
            value_block = v_slots[pl.ds(slot, count), :, columns].reshape(keys_here, value_dim)
            with_ones = jnp.concatenate(
                [value_block, jnp.ones((keys_here, 128), jnp.bfloat16)], axis=1
            )
            for part in (2 * head, 2 * head + 1):
                for begin in range(0, rows, chunk):
                    here = slice(begin, begin + chunk)
                    scores = lax.dot_general(
                        q_masked[part, here],
                        key_block,
                        (((1,), (1,)), ((), ())),
                        preferred_element_type=jnp.float32,
                    )
                    old_peak = peaks[part, here][:, :1]
                    new_peak = jnp.maximum(old_peak, jnp.max(scores, axis=1, keepdims=True))
                    weights = jnp.exp2((scores - new_peak) * exponent_scale)
                    shrink = jnp.exp2((old_peak - new_peak) * exponent_scale)
                    product = jnp.dot(
                        weights.astype(jnp.bfloat16), with_ones, preferred_element_type=jnp.float32
                    )
                    numerators[part, here] = (
                        numerators[part, here] * shrink + product[:, :value_dim]
                    )
                    totals[part, here] = totals[part, here] * shrink + product[:, value_dim:]
                    peaks[part, here] = jnp.broadcast_to(new_peak, (chunk, 128))

    def one_pair(pair, unused):
        slot = 2 * pair + 1

        def pass_on(which, slots, at, target):
            send(slots.at[at], slots, which, at, target).wait_recv()

            @pl.when(at + 2 <= last - 1)
            def _():
                send(slots.at[at], slots, which, at + 2, target).start()

        for which, slots in ((0, k_slots), (1, v_slots)):
            pass_on(which, slots, slot, right)
            if which == 0:

                @pl.when(slot == last - 2)
                def _():
                    send(slots.at[slot], slots, which, last, right).start()

            pass_on(which, slots, slot + 1, left)
            if which == 1:

                @pl.when(slot == last - 2)
                def _():
                    send(slots.at[slot + 1], slots, which, last, left).start()

        absorb(slot, 2)
        return unused

    absorb(0, 1)
    lax.fori_loop(0, (group - 2) // 2, one_pair, 0)
    if last:
        send(k_slots.at[last], k_slots, 0, last, right).wait_recv()
        send(v_slots.at[last], v_slots, 1, last, left).wait_recv()
        absorb(last, 1)

    gain = gain_ref[...] * OUT_SCALE
    for head in range(heads):
        first = numerators[2 * head] / totals[2 * head][:, :1]
        second = numerators[2 * head + 1] / totals[2 * head + 1][:, :1]
        combined = first - lam_ref[head] * second
        mean_square = jnp.mean(combined * combined, axis=1, keepdims=True)
        made[:, head * value_dim : (head + 1) * value_dim] = (
            combined * lax.rsqrt(mean_square + EPSILON) * gain
        ).astype(jnp.bfloat16)

    dev_rows = residual_ref.shape[0]

    def row_copy(step, owner, target):
        return pltpu.make_async_remote_copy(
            src_ref=made.at[pl.ds(pl.multiple_of(target * dev_rows, dev_rows), dev_rows)],
            dst_ref=came.at[owner],
            send_sem=row_send.at[step],
            recv_sem=row_recv.at[step],
            device_id={"tp": target},
            device_id_type=MESH,
        )

    sends = [row_copy(step, me_tp, lax.rem(me_tp + step, tp)) for step in range(1, tp)]
    for copy in sends:
        copy.start()
    came[me_tp] = made[pl.ds(pl.multiple_of(me_tp * dev_rows, dev_rows), dev_rows)]
    load_w_out.wait()
    for step in range(1, tp):
        row_copy(
            step, lax.rem(me_tp + tp - step, tp), lax.rem(me_tp + step, tp)
        ).wait_recv()
    attended = jnp.concatenate([came[peer] for peer in range(tp)], axis=1)
    mixed = jnp.dot(attended, w_out_here[...], preferred_element_type=jnp.float32).astype(
        jnp.bfloat16
    )
    carried = (residual_ref[...].astype(jnp.float32) + mixed.astype(jnp.float32)).astype(
        jnp.bfloat16
    )
    carried_ref[...] = carried
    wide = carried.astype(jnp.float32)
    spread = jnp.mean(wide * wide, axis=1, keepdims=True)
    normed_ref[...] = (wide * lax.rsqrt(spread + EPSILON) * norm_gain_ref[...]).astype(
        jnp.bfloat16
    )
    for copy in sends:
        copy.wait_send()
    for slot in range(1, group):
        send(k_ref, k_slots, 0, slot, right).wait_send()
        send(v_ref, v_slots, 1, slot, right).wait_send()
    for copy in far_copies:
        copy.wait()


def attend(queries, keys, values, lambdas, head_gain, w_out, residual_in, norm_gain, gate, up):
    group = min(16, lax.axis_size("sp"))
    tp = lax.axis_size("tp")
    rows, width = queries.shape
    dev_rows, model_width = residual_in.shape
    heads = lambdas.shape[0]
    value_dim = width // heads
    vmem = pl.BlockSpec(memory_space=pltpu.VMEM)
    return pl.pallas_call(
        functools.partial(attention_kernel, group, tp),
        name="attend",
        out_shape=(
            jax.ShapeDtypeStruct((dev_rows, model_width), jnp.bfloat16),
            jax.ShapeDtypeStruct((dev_rows, model_width), jnp.bfloat16),
            jax.ShapeDtypeStruct(gate.shape, jnp.bfloat16),
            jax.ShapeDtypeStruct(up.shape, jnp.bfloat16),
        ),
        in_specs=[
            vmem,
            vmem,
            vmem,
            pl.BlockSpec(memory_space=pltpu.SMEM),
            vmem,
            pl.BlockSpec(memory_space=pl.ANY),
            vmem,
            vmem,
            pl.BlockSpec(memory_space=pl.ANY),
            pl.BlockSpec(memory_space=pl.ANY),
        ],
        out_specs=(
            vmem,
            vmem,
            pl.BlockSpec(memory_space=pl.ANY),
            pl.BlockSpec(memory_space=pl.ANY),
        ),
        scratch_shapes=[
            pltpu.VMEM((group, rows, width), jnp.bfloat16),
            pltpu.VMEM((group, rows, width), jnp.bfloat16),
            pltpu.VMEM((2 * heads, rows, value_dim), jnp.bfloat16),
            pltpu.VMEM((2 * heads, rows, 128), jnp.float32),
            pltpu.VMEM((2 * heads, rows, 128), jnp.float32),
            pltpu.VMEM((2 * heads, rows, value_dim), jnp.float32),
            pltpu.VMEM((rows, width), jnp.bfloat16),
            pltpu.VMEM((tp, dev_rows, width), jnp.bfloat16),
            pltpu.VMEM(w_out.shape, jnp.bfloat16),
            pltpu.SemaphoreType.DMA((2, group)),
            pltpu.SemaphoreType.DMA((2, group)),
            pltpu.SemaphoreType.DMA((tp,)),
            pltpu.SemaphoreType.DMA((tp,)),
            pltpu.SemaphoreType.DMA((3,)),
            pltpu.SemaphoreType.DMA((2,)),
            pltpu.SemaphoreType.DMA((2,)),
        ],
        compiler_params=pltpu.CompilerParams(
            collective_id=0, has_side_effects=True, vmem_limit_bytes=VMEM_BYTES
        ),
        cost_estimate=pl.CostEstimate(
            flops=50_000_000_000, bytes_accessed=16_000_000, transcendentals=8_000_000
        ),
    )(
        queries,
        keys,
        values,
        lambdas,
        head_gain.reshape(1, -1),
        w_out,
        residual_in,
        norm_gain.reshape(1, -1),
        gate,
        up,
    )


def expert_kernel(
    group,
    x_ref,
    carried_ref,
    share_ref,
    gate_ref,
    up_ref,
    down_ref,
    far_gate_ref,
    far_up_ref,
    out_ref,
    x_slots,
    share_slots,
    gates,
    ups,
    downs,
    hidden,
    parts,
    sums_in,
    sums_out,
    send_sems,
    recv_sems,
    sum_send,
    sum_recv,
    load_sems,
    weight_send,
    weight_recv,
):
    rows, width = x_ref.shape
    pieces = gates.shape[0]
    half_rows, half_width = rows // 2, width // 2
    last, half = group - 1, group // 2
    right, left = ring_neighbours(group)
    expert = lax.axis_index("sp")
    me_tp = lax.axis_index("tp")
    near = me_tp + 1 - 2 * lax.rem(me_tp, 2)
    far = lax.rem(me_tp + pieces // 2, pieces)

    barrier = pltpu.get_barrier_semaphore()
    for neighbour in (right, left):
        pl.semaphore_signal(barrier, inc=1, device_id={"sp": neighbour}, device_id_type=MESH)
    for neighbour in (near, far):
        pl.semaphore_signal(barrier, inc=1, device_id={"tp": neighbour}, device_id_type=MESH)
    pl.semaphore_wait(barrier, 4)

    def landing(slot, which):
        return share_slots.at[slot] if which == 2 else x_slots.at[slot, which]

    def send(source, slot, which, target):
        return pltpu.make_async_remote_copy(
            src_ref=source,
            dst_ref=landing(slot, which),
            send_sem=send_sems.at[which, slot],
            recv_sem=recv_sems.at[which, slot],
            device_id={"sp": target},
            device_id_type=MESH,
        )

    def weight_send_to(source, target_ref, index, target):
        return pltpu.make_async_remote_copy(
            src_ref=source,
            dst_ref=target_ref,
            send_sem=weight_send.at[index],
            recv_sem=weight_recv.at[index],
            device_id={"tp": target},
            device_id_type=MESH,
        )

    own = (x_ref.at[pl.ds(0, half_rows)], x_ref.at[pl.ds(half_rows, half_rows)], share_ref)
    for which in range(3):
        send(own[which], 1, which, right).start()
        send(own[which], 2, which, left).start()
    far_down = weight_send_to(down_ref, downs.at[2], 5, far)
    far_down.start()
    near_copies = [
        weight_send_to(gate_ref, gates.at[1], 0, near),
        weight_send_to(far_gate_ref, gates.at[3], 1, near),
        weight_send_to(up_ref, ups.at[1], 2, near),
        weight_send_to(far_up_ref, ups.at[3], 3, near),
        weight_send_to(down_ref, downs.at[1], 4, near),
    ]
    loads = [
        pltpu.make_async_copy(gate_ref, gates.at[0], load_sems.at[0]),
        pltpu.make_async_copy(up_ref, ups.at[0], load_sems.at[1]),
        pltpu.make_async_copy(far_gate_ref, gates.at[2], load_sems.at[2]),
        pltpu.make_async_copy(far_up_ref, ups.at[2], load_sems.at[3]),
        pltpu.make_async_copy(down_ref, downs.at[0], load_sems.at[4]),
    ]
    for copy in near_copies + loads:
        copy.start()
    def make_hidden(x, begin):
        def one_piece(piece, unused):
            gate_proj = jnp.dot(x, gates[piece], preferred_element_type=jnp.float32)
            up_proj = jnp.dot(x, ups[piece], preferred_element_type=jnp.float32)
            silu = gate_proj / (1.0 + jnp.exp(-gate_proj))
            hidden[piece, begin : begin + x.shape[0]] = (silu * up_proj).astype(jnp.bfloat16)
            return unused

        lax.fori_loop(0, pieces, one_piece, 0)

    def share_column(share):
        wanted = lax.broadcasted_iota(jnp.int32, share.shape, 0) == expert
        line = jnp.sum(jnp.where(wanted, share, 0.0), axis=0, keepdims=True)
        down_index = lax.broadcasted_iota(jnp.int32, (rows, rows), 0)
        across_index = lax.broadcasted_iota(jnp.int32, (rows, rows), 1)
        square = jnp.where(down_index == across_index, jnp.broadcast_to(line, (rows, rows)), 0.0)
        return jnp.sum(square, axis=1, keepdims=True)

    tile = width // 4

    def make_parts(slots):
        begin, count = slots[0] * rows, len(slots) * rows
        columns = [share_column(share_ref[...] if slot == 0 else share_slots[slot]) for slot in slots]
        column = jnp.concatenate(columns, axis=0)

        def one_tile(index, unused):
            at = pl.ds(pl.multiple_of(index * tile, tile), tile)
            total = jnp.zeros((count, tile), jnp.float32)
            for piece in range(pieces):
                total = total + lax.dot_general(
                    hidden[piece, begin : begin + count],
                    downs[piece, at, :],
                    (((1,), (1,)), ((), ())),
                    preferred_element_type=jnp.float32,
                )
            parts[begin : begin + count, at] = total.astype(jnp.bfloat16).astype(jnp.float32) * column
            return unused

        lax.fori_loop(0, 4, one_tile, 0)

    def exchange(step):
        ahead, behind = 2 * step - 1, 2 * step
        for which in range(3):
            send(landing(ahead, which), ahead, which, right).wait_recv()
            if step < half - 1:
                send(landing(ahead, which), ahead + 2, which, right).start()
            elif which != 1:
                send(landing(ahead, which), last, which, right).start()
            send(landing(behind, which), behind, which, left).wait_recv()
            if step < half - 1:
                send(landing(behind, which), behind + 2, which, left).start()
            elif which == 1:
                send(landing(behind, which), last, which, left).start()

    def sum_copy(side, step, chunk):
        return pltpu.make_async_remote_copy(
            src_ref=sums_out.at[side, step, chunk],
            dst_ref=sums_in.at[side, step, chunk],
            send_sem=sum_send.at[side, step, chunk],
            recv_sem=sum_recv.at[side, step, chunk],
            device_id={"sp": left if side else right},
            device_id_type=MESH,
        )

    def part_of(side, slot, chunk):
        begin = slot * rows + chunk * half_rows
        return parts[begin : begin + half_rows, side * half_width : (side + 1) * half_width]

    def sum_step(step):
        for chunk in range(2):
            for side in range(2):
                if step < half:
                    slot = 2 * step - 1 + side
                elif step == half:
                    slot = last
                else:
                    slot = 2 * (group - step) - side
                value = part_of(side, slot, chunk)
                if step > 1:
                    sum_copy(side, step - 1, chunk).wait_recv()
                    value = value + sums_in[side, step - 1, chunk].astype(jnp.float32)
                sums_out[side, step, chunk] = value.astype(jnp.bfloat16)
                sum_copy(side, step, chunk).start()

    def pair_hidden(step):
        pair = jnp.concatenate(
            [x_slots[slot, part] for slot in (2 * step - 1, 2 * step) for part in range(2)], axis=0
        )
        make_hidden(pair, (2 * step - 1) * rows)

    exchange(1)
    for load in loads:
        load.wait()
    for copy in near_copies:
        copy.wait_recv()
    pair_hidden(1)
    if half > 2:
        exchange(2)
        pair_hidden(2)
    far_down.wait_recv()
    near_down = weight_send_to(downs.at[2], downs.at[3], 6, near)
    near_down.start()
    near_down.wait_recv()
    make_parts((1, 2))
    for step in range(3, half):
        exchange(step)
        sum_step(step - 2)
        make_parts((2 * step - 3, 2 * step - 2))
        pair_hidden(step)
    if half > 2:
        sum_step(half - 2)
        make_parts((last - 2, last - 1))
    send(landing(last, 0), last, 0, right).wait_recv()
    send(landing(last, 1), last, 1, left).wait_recv()
    send(landing(last, 2), last, 2, right).wait_recv()
    sum_step(half - 1)
    make_hidden(jnp.concatenate([x_slots[last, 0], x_slots[last, 1]], axis=0), last * rows)
    make_parts((last,))
    for step in range(half, group):
        sum_step(step)
        if step == half:
            make_hidden(x_ref[...], 0)
        if step == min(half + 1, last):
            make_parts((0,))
    for chunk in range(2):
        here = slice(chunk * half_rows, (chunk + 1) * half_rows)
        for side in range(2):
            there = slice(side * half_width, (side + 1) * half_width)
            sum_copy(side, last, chunk).wait_recv()
            out_ref[here, there] = (
                carried_ref[here, there].astype(jnp.float32)
                + (part_of(side, 0, chunk) + sums_in[side, last, chunk].astype(jnp.float32))
            ).astype(jnp.bfloat16)
    for slot in range(1, group):
        for which in range(3):
            send(landing(slot, which), slot, which, right).wait_send()
    for step in range(1, group):
        for side in range(2):
            for chunk in range(2):
                sum_copy(side, step, chunk).wait_send()
    for copy in near_copies + [far_down, near_down]:
        copy.wait_send()


def expert_layer(normed, carried, shares, gate, up, down, far_gate, far_up):
    group = lax.axis_size("sp")
    pieces = lax.axis_size("tp")
    rows, width = normed.shape
    units = gate.shape[1]
    vmem = pl.BlockSpec(memory_space=pltpu.VMEM)
    outside = pl.BlockSpec(memory_space=pl.ANY)
    bf16 = jnp.bfloat16
    return pl.pallas_call(
        functools.partial(expert_kernel, group),
        name="experts",
        out_shape=jax.ShapeDtypeStruct((rows, width), bf16),
        in_specs=[vmem] * 3 + [outside] * 5,
        out_specs=vmem,
        scratch_shapes=[
            pltpu.VMEM((group, 2, rows // 2, width), bf16),
            pltpu.VMEM((group,) + shares.shape, jnp.float32),
            pltpu.VMEM((pieces, width, units), bf16),
            pltpu.VMEM((pieces, width, units), bf16),
            pltpu.VMEM((pieces, width, units), bf16),
            pltpu.VMEM((pieces, group * rows, units), bf16),
            pltpu.VMEM((group * rows, width), jnp.float32),
            pltpu.VMEM((2, group, 2, rows // 2, width // 2), bf16),
            pltpu.VMEM((2, group, 2, rows // 2, width // 2), bf16),
            pltpu.SemaphoreType.DMA((3, group)),
            pltpu.SemaphoreType.DMA((3, group)),
            pltpu.SemaphoreType.DMA((2, group, 2)),
            pltpu.SemaphoreType.DMA((2, group, 2)),
            pltpu.SemaphoreType.DMA((5,)),
            pltpu.SemaphoreType.DMA((7,)),
            pltpu.SemaphoreType.DMA((7,)),
        ],
        compiler_params=pltpu.CompilerParams(
            collective_id=1, has_side_effects=True, vmem_limit_bytes=VMEM_BYTES
        ),
    )(normed, carried, shares, gate, up, down, far_gate, far_up)


def nearest_first(position, count, nth):
    order = [
        sorted(range(count), key=lambda other: (abs(other - here), other if 2 * here < count else -other))
        for here in range(count)
    ]
    chosen = jnp.int32(order[0][nth])
    for here in range(1, count):
        chosen = jnp.where(position == here, order[here][nth], chosen)
    return chosen


class WeightFlow:
    def __init__(self, chunks, refs, pieces, send_sems, recv_sems, load_sems):
        gate_ref, up_ref, down_ref = refs
        gates, ups, downs = pieces
        me_tp, tp = lax.axis_index("tp"), lax.axis_size("tp")
        near = me_tp + 1 - 2 * lax.rem(me_tp, 2)
        far = lax.rem(me_tp + tp // 2, tp)
        width = gate_ref.shape[0]
        first, tile = 3 * width // 8, width // chunks
        self.used = 0

        def to(target, source, landing):
            index = self.used
            self.used += 1
            return pltpu.make_async_remote_copy(
                src_ref=source,
                dst_ref=landing,
                send_sem=send_sems.at[index],
                recv_sem=recv_sems.at[index],
                device_id={"tp": target},
                device_id_type=MESH,
            )

        cuts = [(0, pl.ds(0, width)), (1, pl.ds(0, first)), (1, pl.ds(first, width - first))]
        cuts += [(2, pl.ds(chunk * tile, tile)) for chunk in range(chunks)]
        self.far = [to(far, refs[kind].at[at], pieces[kind].at[2, at]) for kind, at in cuts]
        self.relays = [to(near, pieces[kind].at[2, at], pieces[kind].at[3, at]) for kind, at in cuts]
        self.near = [to(near, refs[kind], pieces[kind].at[1]) for kind in range(3)]
        self.loads = [
            pltpu.make_async_copy(refs[kind], pieces[kind].at[0], load_sems.at[kind])
            for kind in range(3)
        ]

    def start_far(self, phase):
        if phase == 0:
            for copy in self.far[:2]:
                copy.start()
        else:
            for copy in self.far[2:] + self.near + self.loads:
                copy.start()

    def pass_first(self):
        for far, relay in zip(self.far[:2], self.relays[:2]):
            far.wait_recv()
            relay.start()

    def hidden_ready(self):
        self.far[2].wait_recv()
        self.relays[2].start()
        for copy in self.loads:
            copy.wait()
        for copy in self.near + self.relays[:3]:
            copy.wait_recv()

    def down_ready(self, chunk):
        self.far[3 + chunk].wait_recv()
        self.relays[3 + chunk].start()
        self.relays[3 + chunk].wait_recv()

    def finish(self):
        for copy in self.far + self.relays + self.near:
            copy.wait_send()


def attention_part(
    sides,
    cores,
    start_far,
    q_ref,
    k_ref,
    v_ref,
    lam_ref,
    gain_ref,
    w_out_ref,
    residual_ref,
    norm_gain_ref,
    carried_ref,
    normed_ref,
    q_here,
    kv,
    q_masked,
    peaks,
    totals,
    numerators,
    made,
    came,
    lam_all,
    w_out_here,
    residual_here,
    in_send,
    q_recv,
    kv_recv,
    pair_send,
    side_send,
    lam_sems,
    row_send,
    row_recv,
    load_sems,
):
    rows, width = q_ref.shape
    depth = kv.shape[2]
    heads = width // 128
    value_dim = width // heads
    head_dim = value_dim // 2
    half = rows // cores
    exponent_scale = head_dim ** (-0.5) * math.log2(math.e)
    me_sp, me_tp = lax.axis_index("sp"), lax.axis_index("tp")
    tp = lax.axis_size("tp")
    z, y = lax.div(me_sp, sides), lax.rem(me_sp, sides)
    x, c = lax.div(me_tp, cores), lax.rem(me_tp, cores)
    other_y, other_c = 1 - y, 1 - c

    def device(at_z, at_y, at_x, at_c):
        return {"sp": at_z * sides + at_y, "tp": at_x * cores + at_c}

    lam_row = lax.broadcasted_iota(jnp.int32, lam_all.shape[1:], 0)
    lam_block = jnp.zeros(lam_all.shape[1:], jnp.float32)
    for head in range(heads):
        lam_block = jnp.where(lam_row == head, lam_ref[head], lam_block)
    lam_all[c] = lam_block

    barrier = pltpu.get_barrier_semaphore()
    plane = depth * tp
    spot = z * tp + me_tp
    for step in range(1, plane):
        peer = lax.rem(spot + step, plane)
        pl.semaphore_signal(
            barrier,
            inc=1,
            device_id={"sp": lax.div(peer, tp) * sides + y, "tp": lax.rem(peer, tp)},
            device_id_type=MESH,
        )
    pl.semaphore_signal(barrier, inc=1, device_id=device(z, other_y, x, c), device_id_type=MESH)
    pl.semaphore_wait(barrier, plane)

    def remote(source, landing, send_sem, recv_sem, target):
        return pltpu.make_async_remote_copy(
            src_ref=source,
            dst_ref=landing,
            send_sem=send_sem,
            recv_sem=recv_sem,
            device_id=target,
            device_id_type=MESH,
        )

    def deliver(source, landing, send_sem, recv_sem, target, stays):
        @pl.when(stays)
        def _():
            pltpu.make_async_copy(source, landing, recv_sem).start()

        @pl.when(jnp.logical_not(stays))
        def _():
            remote(source, landing, send_sem, recv_sem, target).start()

    def left(source, landing, send_sem, recv_sem, target, stays):
        @pl.when(jnp.logical_not(stays))
        def _():
            remote(source, landing, send_sem, recv_sem, target).wait_send()

    inputs = []
    for head in range(heads):
        columns = slice(head * value_dim, (head + 1) * value_dim)
        to_z = c * heads + head
        for core in range(cores):
            inputs.append(
                (
                    q_ref.at[core * half : (core + 1) * half, columns],
                    q_here.at[z],
                    in_send.at[head, core],
                    q_recv.at[z],
                    device(to_z, y, x, core),
                    jnp.logical_and(to_z == z, c == core),
                )
            )
    for head in range(heads):
        columns = slice(head * value_dim, (head + 1) * value_dim)
        to_z = c * heads + head
        for core, source in ((0, k_ref), (1, v_ref)):
            inputs.append(
                (
                    source.at[:, columns],
                    kv.at[core, y, z],
                    in_send.at[head, cores + core],
                    kv_recv.at[core, y, z],
                    device(to_z, y, x, core),
                    jnp.logical_and(to_z == z, c == core),
                )
            )
    lam_copy = remote(lam_all.at[c], lam_all.at[c], lam_sems.at[0], lam_sems.at[1], device(z, y, x, other_c))
    for item in inputs:
        deliver(*item)
    lam_copy.start()
    start_far(0)
    load_w_out = pltpu.make_async_copy(w_out_ref, w_out_here, load_sems.at[0])
    load_w_out.start()
    load_residual = pltpu.make_async_copy(residual_ref, residual_here, load_sems.at[1])
    load_residual.start()

    peaks[...] = jnp.full(peaks.shape, FLOOR_SCORE, jnp.float32)
    totals[...] = jnp.zeros(totals.shape, jnp.float32)
    numerators[...] = jnp.zeros(numerators.shape, jnp.float32)

    def block_wait(tensor, side, at):
        slot = kv.at[tensor, side, at]
        remote(
            slot, slot, pair_send.at[0, 0], kv_recv.at[tensor, side, at], device(z, other_y, x, c)
        ).wait_recv()

    def to_pair(side, at):
        slot = kv.at[c, side, at]
        return remote(
            slot, slot, pair_send.at[side, at], kv_recv.at[c, side, at], device(z, y, x, other_c)
        )

    def to_side(at):
        slot = kv.at[c, y, at]
        return remote(
            slot, slot, side_send.at[at], kv_recv.at[c, y, at], device(z, other_y, x, c)
        )

    def take_own(at):
        block_wait(c, y, at)
        to_side(at).start()
        to_pair(y, at).start()

    def take_side(at):
        block_wait(c, other_y, at)
        to_pair(other_y, at).start()

    def absorb(places, part):
        if part == 0:
            for side, at in places:
                block_wait(other_c, side, at)
        key_block = jnp.concatenate([kv[0, side, at] for side, at in places], axis=0)
        value_block = jnp.concatenate([kv[1, side, at] for side, at in places], axis=0)
        count = len(places) * rows
        with_ones = jnp.concatenate([value_block, jnp.ones((count, 128), jnp.bfloat16)], axis=1)

        def scores_of(begin):
            return lax.dot_general(
                q_masked[part, begin : begin + half],
                key_block,
                (((1,), (1,)), ((), ())),
                preferred_element_type=jnp.float32,
            )

        coming = scores_of(0)
        for begin in range(0, depth * half, half):
            here = slice(begin, begin + half)
            scores = coming
            if begin + half < depth * half:
                coming = scores_of(begin + half)
            old_peak = peaks[part, here]
            row_peak = jnp.broadcast_to(jnp.max(scores, axis=1, keepdims=True), (half, 128))
            new_peak = jnp.maximum(old_peak, row_peak)
            level = jnp.concatenate([new_peak] * (count // 128), axis=1)
            weights = jnp.exp2((scores - level) * exponent_scale)
            shrink = jnp.exp2((old_peak - new_peak) * exponent_scale)
            product = jnp.dot(
                weights.astype(jnp.bfloat16), with_ones, preferred_element_type=jnp.float32
            )
            numerators[part, here] = numerators[part, here] * shrink + product[:, :value_dim]
            totals[part, here] = totals[part, here] * shrink + product[:, value_dim:]
            peaks[part, here] = new_peak

    take_own(z)
    take_side(z)
    lane = lax.broadcasted_iota(jnp.int32, (half, value_dim), 1)
    for at in range(depth):
        remote(
            q_here.at[at], q_here.at[at], pair_send.at[0, 0], q_recv.at[at], device(z, other_y, x, c)
        ).wait_recv()
        both = q_here[at]
        here = slice(at * half, (at + 1) * half)
        q_masked[0, here] = jnp.where(lane < head_dim, both, jnp.zeros_like(both))
        q_masked[1, here] = jnp.where(lane >= head_dim, both, jnp.zeros_like(both))

    def nth(index):
        chosen = nearest_first(z, depth, 0)
        for place in range(1, depth):
            chosen = jnp.where(index == place, nearest_first(z, depth, place), chosen)
        return chosen

    absorb([(y, z)], 0)
    take_own(nth(1))
    absorb([(y, z)], 1)

    def one_block(index, unused):
        at, before = nth(index), nth(index - 1)
        absorb([(y, at), (other_y, before)], 0)

        @pl.when(index < depth - 1)
        def _():
            take_own(nth(index + 1))

        take_side(at)
        absorb([(y, at), (other_y, before)], 1)
        return unused

    lax.fori_loop(1, depth, one_block, 0)
    last = nth(depth - 1)
    absorb([(other_y, last)], 0)
    absorb([(other_y, last)], 1)

    lam_copy.wait_recv()
    lam_here = lam_all[lax.div(z, heads)]
    lam = jnp.sum(jnp.where(lam_row == lax.rem(z, heads), lam_here, 0.0), axis=0, keepdims=True)
    gain = gain_ref[...] * OUT_SCALE
    dev_rows = residual_ref.shape[0]
    my_head = x * depth + z

    def row_item(at, part):
        return (
            made.at[at, part * dev_rows : (part + 1) * dev_rows],
            came.at[my_head],
            row_send.at[at, part],
            row_recv.at[my_head],
            device(at, y, c, part),
            jnp.logical_and(at == z, jnp.logical_and(x == c, c == part)),
        )

    for place in reversed(range(depth)):
        at = nearest_first(z, depth, place)
        here = pl.ds(pl.multiple_of(at * half, half), half)
        first = numerators[0, here] / totals[0, here][:, :1]
        second = numerators[1, here] / totals[1, here][:, :1]
        combined = first - lam * second
        mean_square = jnp.mean(combined * combined, axis=1, keepdims=True)
        made[at] = (combined * lax.rsqrt(mean_square + EPSILON) * gain).astype(jnp.bfloat16)
        for part in range(half // dev_rows):
            deliver(*row_item(at, part))
    start_far(1)
    load_w_out.wait()
    load_residual.wait()
    for head in range(came.shape[0]):
        remote(
            came.at[head], came.at[head], pair_send.at[0, 0], row_recv.at[head], device(z, other_y, x, c)
        ).wait_recv()
    attended = jnp.concatenate([came[head] for head in range(came.shape[0])], axis=1)
    mixed = jnp.dot(attended, w_out_here[...], preferred_element_type=jnp.float32).astype(
        jnp.bfloat16
    )
    carried = (residual_here[...].astype(jnp.float32) + mixed.astype(jnp.float32)).astype(
        jnp.bfloat16
    )
    carried_ref[...] = carried
    wide = carried.astype(jnp.float32)
    spread = jnp.mean(wide * wide, axis=1, keepdims=True)
    normed_ref[...] = (wide * lax.rsqrt(spread + EPSILON) * norm_gain_ref[...]).astype(
        jnp.bfloat16
    )

    def finish():
        for item in inputs:
            left(*item)
        lam_copy.wait_send()
        for at in range(depth):
            to_side(at).wait_send()
            to_pair(0, at).wait_send()
            to_pair(1, at).wait_send()
            for part in range(half // dev_rows):
                left(*row_item(at, part))

    return finish


def expert_part(
    sides,
    weights,
    x_ref,
    carried_ref,
    share_ref,
    out_ref,
    x_all,
    share_all,
    selections,
    columns,
    takes,
    picked,
    packed_out,
    gates,
    ups,
    downs,
    hidden,
    results_out,
    results_in,
    results_own,
    parts,
    sums_in,
    sums_out,
    out_here,
    out_sems,
    x_send,
    x_recv,
    share_send,
    share_recv,
    pack_send,
    pack_recv,
    result_send,
    result_recv,
    sum_send,
    sum_recv,
):
    rows, width = x_ref.shape
    depth = x_all.shape[0]
    capacity = rows // 2
    pieces = gates.shape[0]
    chunks = x_recv.shape[1]
    tile = width // chunks
    splits = sum_send.shape[1] // chunks
    fine_tile = tile // splits
    me_sp, me_tp = lax.axis_index("sp"), lax.axis_index("tp")
    z, y = lax.div(me_sp, sides), lax.rem(me_sp, sides)
    partner = z * sides + 1 - y
    has_below, has_above = z > 0, z < depth - 1
    middle = jnp.logical_and(has_below, has_above)
    blocks = [nearest_first(z, depth, place) for place in range(depth)]

    def remote(source, landing, send_sem, recv_sem, target):
        return pltpu.make_async_remote_copy(
            src_ref=source,
            dst_ref=landing,
            send_sem=send_sem,
            recv_sem=recv_sem,
            device_id=target,
            device_id_type=MESH,
        )

    below, above = {"sp": me_sp - sides}, {"sp": me_sp + sides}

    def cut(chunk):
        return pl.ds(chunk * tile, tile)

    def x_copy(source, block, chunk, downward):
        return remote(
            source.at[:, cut(chunk)],
            x_all.at[block, :, cut(chunk)],
            x_send.at[downward, block, chunk],
            x_recv.at[block, chunk],
            below if downward else above,
        )

    def share_copy(source, block, downward):
        return remote(
            source,
            share_all.at[block],
            share_send.at[downward, block],
            share_recv.at[block],
            below if downward else above,
        )

    for downward, exists in ((0, has_above), (1, has_below)):

        @pl.when(exists)
        def _():
            share_copy(share_ref, z, downward).start()
            for chunk in range(chunks):
                x_copy(x_ref, z, chunk, downward).start()

    def to_far(index, source, landing):
        return remote(source, landing, weight_send.at[index], weight_recv.at[index], {"tp": far})

    def to_near(index, source, landing):
        return remote(source, landing, weight_send.at[index], weight_recv.at[index], {"tp": near})

    def select(step, share):
        named = (share > 0.0).astype(jnp.float32)
        earlier = lax.broadcasted_iota(jnp.int32, (rows, rows), 0) < lax.broadcasted_iota(
            jnp.int32, (rows, rows), 1
        )
        rank = jnp.dot(
            named.astype(jnp.bfloat16),
            earlier.astype(jnp.float32).astype(jnp.bfloat16),
            preferred_element_type=jnp.float32,
        )
        expert_row = lax.broadcasted_iota(jnp.int32, share.shape, 0)
        slot = lax.broadcasted_iota(jnp.int32, (capacity, rows), 0).astype(jnp.float32)
        diagonal = lax.broadcasted_iota(jnp.int32, (rows, rows), 0) == lax.broadcasted_iota(
            jnp.int32, (rows, rows), 1
        )
        found = []
        for side, expert in enumerate((partner, me_sp)):

            def line(table):
                return jnp.sum(jnp.where(expert_row == expert, table, 0.0), axis=0, keepdims=True)

            taken = jnp.where(jnp.logical_and(slot == line(rank), line(named) > 0.0), 1.0, 0.0)
            found.append(taken)
            selections[step, side] = taken.T.astype(jnp.bfloat16)
            square = jnp.where(diagonal, jnp.broadcast_to(line(share), (rows, rows)), 0.0)
            columns[step, side] = jnp.broadcast_to(
                jnp.sum(square, axis=1, keepdims=True), (rows, 128)
            )
        return jnp.concatenate(found, axis=0).astype(jnp.bfloat16)

    def pack_copy(step, chunk):
        return remote(
            packed_out.at[step, :, cut(chunk)],
            picked.at[pl.ds(step * rows, capacity), cut(chunk)],
            pack_send.at[step, chunk],
            pack_recv.at[step, chunk],
            {"sp": partner},
        )

    def pack(step, chunk):
        block = x_ref[:, cut(chunk)] if step == 0 else x_all[blocks[step], :, cut(chunk)]
        compact = jnp.dot(takes[step], block, preferred_element_type=jnp.float32).astype(jnp.bfloat16)
        packed_out[step, :, cut(chunk)] = compact[:capacity]
        picked[step * rows + capacity : (step + 1) * rows, cut(chunk)] = compact[capacity:]
        pack_copy(step, chunk).start()

    def forward(step, chunk):
        block = blocks[step]
        go_up = jnp.logical_and(block < z, has_above)
        go_down = jnp.logical_and(block > z, has_below)
        if chunk == 0:
            share_copy(share_all.at[block], block, 0).wait_recv()
        x_copy(x_all.at[block], block, chunk, 0).wait_recv()
        for downward, goes in ((0, go_up), (1, go_down)):

            @pl.when(goes)
            def _():
                if chunk == 0:
                    share_copy(share_all.at[block], block, downward).start()
                x_copy(x_all.at[block], block, chunk, downward).start()

    def choose(step):
        takes[step] = select(step, share_ref[...] if step == 0 else share_all[blocks[step]])

    def pack_all(step):
        choose(step)
        for chunk in range(chunks):
            pack(step, chunk)

    def bring(step, chunk):
        forward(step, chunk)
        if chunk == 0:
            choose(step)
        pack(step, chunk)

    def make_hidden(first, last, piece):
        here = slice(first * rows, last * rows)
        x = picked[here]
        gate_proj = jnp.dot(x, gates[piece], preferred_element_type=jnp.float32)
        up_proj = jnp.dot(x, ups[piece], preferred_element_type=jnp.float32)
        silu = gate_proj / (1.0 + jnp.exp(-gate_proj))
        hidden[piece, here] = (silu * up_proj).astype(jnp.bfloat16)

    def result_copy(step, chunk):
        return remote(
            results_out.at[step, :, cut(chunk)],
            results_in.at[step, :, cut(chunk)],
            result_send.at[step, chunk],
            result_recv.at[step, chunk],
            {"sp": partner},
        )

    def make_results(first, last, chunk):
        total = jnp.zeros(((last - first) * rows, tile), jnp.float32)
        for piece in range(pieces):
            total = total + lax.dot_general(
                hidden[piece, first * rows : last * rows],
                downs[piece, cut(chunk)],
                (((1,), (1,)), ((), ())),
                preferred_element_type=jnp.float32,
            )
        total = total.astype(jnp.bfloat16)
        for step in range(first, last):
            at = (step - first) * rows
            results_out[step, :, cut(chunk)] = total[at : at + capacity]
            results_own[step, :, cut(chunk)] = total[at + capacity : at + rows]
            result_copy(step, chunk).start()

    def spread(step, chunk):
        result_copy(step, chunk).wait_recv()
        theirs = jnp.dot(
            selections[step, 0], results_in[step, :, cut(chunk)], preferred_element_type=jnp.float32
        )
        ours = jnp.dot(
            selections[step, 1], results_own[step, :, cut(chunk)], preferred_element_type=jnp.float32
        )
        parts[step, :, cut(chunk)] = theirs * columns[step, 0][:, :1] + ours * columns[step, 1][:, :1]

    def fine_cut(chunk):
        return pl.ds(chunk * fine_tile, fine_tile)

    def sum_copy(step, chunk, downward):
        block = blocks[step]
        return remote(
            sums_out.at[step, :, fine_cut(chunk)],
            sums_in.at[downward, block, :, fine_cut(chunk)],
            sum_send.at[step, chunk],
            sum_recv.at[downward, block, chunk],
            below if downward else above,
        )

    def pass_sum(step, chunk, has_outer):
        pass_fine(step, range(chunk * splits, (chunk + 1) * splits), has_outer)

    def pass_fine(step, fines, has_outer):
        block = blocks[step]
        for downward, goes in ((0, block > z), (1, block < z)):

            @pl.when(goes)
            def _():
                for fine in fines:
                    value = parts[step, :, fine_cut(fine)]
                    if has_outer:
                        sum_copy(step, fine, downward).wait_recv()
                        value = value + sums_in[downward, block, :, fine_cut(fine)].astype(jnp.float32)
                    sums_out[step, :, fine_cut(fine)] = value.astype(jnp.bfloat16)
                    sum_copy(step, fine, downward).start()

    def at_end(action):
        pl.when(jnp.logical_not(middle))(action)

    def at_middle(action):
        pl.when(middle)(action)

    def packed(step):
        for chunk in range(chunks):
            pack_copy(step, chunk).wait_recv()

    def all_hidden(step):
        for piece in range(pieces):
            make_hidden(step, step + 1, piece)

    def settle(step, chunk):
        spread(step, chunk)
        at_end(functools.partial(pass_sum, step, chunk, False))

    def second(chunk):
        at_end(functools.partial(bring, 2, chunk))
        at_middle(functools.partial(bring, 3, chunk))

    def third(chunk):
        at_end(functools.partial(bring, 3, chunk))

    pack_all(0)
    weights.pass_first()
    for chunk in range(chunks):
        bring(1, chunk)
        at_middle(functools.partial(forward, 2, chunk))
    at_middle(functools.partial(pack_all, 2))
    weights.hidden_ready()
    second(0)
    packed(1)
    all_hidden(1)
    second(1)
    weights.down_ready(0)
    make_results(1, 2, 0)
    second(2)
    weights.down_ready(1)
    make_results(1, 2, 1)
    second(3)
    settle(1, 0)
    packed(2)
    all_hidden(2)
    make_results(2, 3, 0)
    make_results(2, 3, 1)
    third(0)
    settle(1, 1)
    third(1)
    weights.down_ready(2)
    make_results(1, 3, 2)
    third(2)
    settle(2, 0)
    settle(2, 1)
    third(3)
    weights.down_ready(3)
    make_results(1, 3, 3)
    settle(1, 2)
    settle(2, 2)
    packed(3)
    all_hidden(3)
    for chunk in range(chunks):
        make_results(3, 4, chunk)
    settle(1, 3)
    settle(2, 3)
    def finish_own():
        packed(0)
        all_hidden(0)
        for chunk in range(chunks):
            make_results(0, 1, chunk)

    at_middle(finish_own)
    for chunk in range(chunks):
        at_middle(functools.partial(pass_sum, 2, chunk, True))
    for chunk in range(chunks):
        spread(3, chunk)
        at_end(functools.partial(pass_sum, 3, chunk, False))
    at_end(finish_own)

    @at_middle
    def _():
        lag, fines = 3, chunks * splits
        for fine in range(fines + lag):
            if fine < fines:
                pass_fine(3, (fine,), True)
            if fine >= lag:
                pass_fine(1, (fine - lag,), True)

    stores = []
    for chunk in range(chunks):
        spread(0, chunk)
    for chunk in range(chunks):
        here = cut(chunk)

        def arrived(downward):
            for fine in range(chunk * splits, (chunk + 1) * splits):
                there = fine_cut(fine)
                landing = sums_in.at[downward, z, :, there]
                remote(
                    landing, landing, sum_send.at[0, fine], sum_recv.at[downward, z, fine], above
                ).wait_recv()
                parts[0, :, there] = parts[0, :, there] + sums_in[downward, z, :, there].astype(
                    jnp.float32
                )

        pl.when(has_below)(functools.partial(arrived, 0))
        pl.when(has_above)(functools.partial(arrived, 1))
        out_here[:, here] = (carried_ref[:, here].astype(jnp.float32) + parts[0, :, here]).astype(
            jnp.bfloat16
        )
        stores.append(pltpu.make_async_copy(out_here.at[:, here], out_ref.at[:, here], out_sems.at[chunk]))
        stores[-1].start()

    for downward, exists in ((0, has_above), (1, has_below)):

        @pl.when(exists)
        def _():
            share_copy(share_ref, z, downward).wait_send()
            for chunk in range(chunks):
                x_copy(x_ref, z, chunk, downward).wait_send()

    for step in range(1, depth):
        block = blocks[step]
        for downward, goes in (
            (0, jnp.logical_and(block < z, has_above)),
            (1, jnp.logical_and(block > z, has_below)),
        ):

            @pl.when(goes)
            def _():
                share_copy(share_all.at[block], block, downward).wait_send()
                for chunk in range(chunks):
                    x_copy(x_all.at[block], block, chunk, downward).wait_send()

    for step in range(depth):
        for chunk in range(chunks):
            pack_copy(step, chunk).wait_send()
            result_copy(step, chunk).wait_send()
        if step:
            for chunk in range(chunks * splits):
                sum_copy(step, chunk, 0).wait_send()

    return stores


def layer_kernel(sides, cores, chunks, *refs):
    inputs, rest = refs[:8], refs[8:]
    ids_ref, shares_ref, gate_ref, up_ref, down_ref, out_ref = rest[:6]
    carried, normed, share_here = rest[6:9]
    attention_scratch, rest = rest[9:29], rest[29:]
    dev_rows, routes = ids_ref.shape
    lane = lax.broadcasted_iota(jnp.int32, (dev_rows, 128), 1)
    table = jnp.zeros((dev_rows, 128), jnp.float32)
    for route in range(routes):
        hit = ids_ref[:, route : route + 1] == lane
        table = table + jnp.where(hit, shares_ref[:, route : route + 1], 0.0)
    share_here[...] = table.T[: share_here.shape[0]]
    expert_scratch, (weight_send, weight_recv, weight_loads) = rest[:-3], rest[-3:]
    weights = WeightFlow(
        chunks,
        (gate_ref, up_ref, down_ref),
        expert_scratch[7:10],
        weight_send,
        weight_recv,
        weight_loads,
    )
    finish = attention_part(
        sides, cores, weights.start_far, *inputs, carried, normed, *attention_scratch
    )
    stores = expert_part(sides, weights, normed, carried, share_here, out_ref, *expert_scratch)
    finish()
    weights.finish()
    for copy in stores:
        copy.wait()


def whole_layer(
    queries,
    keys,
    values,
    lambdas,
    head_gain,
    w_out,
    residual_in,
    norm_gain,
    route_ids,
    route_weight,
    gate,
    up,
    down,
):
    tp = lax.axis_size("tp")
    sides, cores, chunks = 2, 2, 4
    experts = lax.axis_size("sp")
    depth = experts // sides
    rows, width = queries.shape
    dev_rows, model_width = residual_in.shape
    units = gate.shape[1]
    value_dim = 128
    heads_all = (width // value_dim) * tp
    half = rows // cores
    capacity = dev_rows // 2
    vmem = pl.BlockSpec(memory_space=pltpu.VMEM)
    smem = pl.BlockSpec(memory_space=pltpu.SMEM)
    outside = pl.BlockSpec(memory_space=pl.ANY)
    bf16, f32 = jnp.bfloat16, jnp.float32
    dma = pltpu.SemaphoreType.DMA
    attention_scratch = [
        pltpu.VMEM((depth, half, value_dim), bf16),
        pltpu.VMEM((2, sides, depth, rows, value_dim), bf16),
        pltpu.VMEM((2, depth * half, value_dim), bf16),
        pltpu.VMEM((2, depth * half, 128), f32),
        pltpu.VMEM((2, depth * half, 128), f32),
        pltpu.VMEM((2, depth * half, value_dim), f32),
        pltpu.VMEM((depth, half, value_dim), bf16),
        pltpu.VMEM((heads_all, dev_rows, value_dim), bf16),
        pltpu.VMEM((cores, 8, 128), f32),
        pltpu.VMEM(w_out.shape, bf16),
        pltpu.VMEM(residual_in.shape, bf16),
        dma((width // value_dim, 2 * cores)),
        dma((depth,)),
        dma((2, sides, depth)),
        dma((sides, depth)),
        dma((depth,)),
        dma((2,)),
        dma((depth, half // dev_rows)),
        dma((heads_all,)),
        dma((2,)),
    ]
    expert_scratch = [
        pltpu.VMEM((depth, dev_rows, model_width), bf16),
        pltpu.VMEM((depth, experts, dev_rows), f32),
        pltpu.VMEM((depth, 2, dev_rows, capacity), bf16),
        pltpu.VMEM((depth, 2, dev_rows, 128), f32),
        pltpu.VMEM((depth, dev_rows, dev_rows), bf16),
        pltpu.VMEM((depth * dev_rows, model_width), bf16),
        pltpu.VMEM((depth, capacity, model_width), bf16),
        pltpu.VMEM((tp, model_width, units), bf16),
        pltpu.VMEM((tp, model_width, units), bf16),
        pltpu.VMEM((tp, model_width, units), bf16),
        pltpu.VMEM((tp, depth * dev_rows, units), bf16),
        pltpu.VMEM((depth, capacity, model_width), bf16),
        pltpu.VMEM((depth, capacity, model_width), bf16),
        pltpu.VMEM((depth, capacity, model_width), bf16),
        pltpu.VMEM((depth, dev_rows, model_width), f32),
        pltpu.VMEM((2, depth, dev_rows, model_width), bf16),
        pltpu.VMEM((depth, dev_rows, model_width), bf16),
        pltpu.VMEM((dev_rows, model_width), bf16),
        dma((chunks,)),
        dma((2, depth, chunks)),
        dma((depth, chunks)),
        dma((2, depth)),
        dma((depth,)),
        dma((depth, chunks)),
        dma((depth, chunks)),
        dma((depth, chunks)),
        dma((depth, chunks)),
        dma((depth, 2 * chunks)),
        dma((2, depth, 2 * chunks)),
    ]
    weight_copies = 2 * (chunks + 3) + 3
    return pl.pallas_call(
        functools.partial(layer_kernel, sides, cores, chunks),
        name="layer",
        out_shape=jax.ShapeDtypeStruct((dev_rows, model_width), bf16),
        in_specs=[outside] * 3 + [smem, vmem, outside, outside] + [vmem] * 3 + [outside] * 3,
        out_specs=outside,
        scratch_shapes=[
            pltpu.VMEM((dev_rows, model_width), bf16),
            pltpu.VMEM((dev_rows, model_width), bf16),
            pltpu.VMEM((experts, dev_rows), f32),
        ]
        + attention_scratch
        + expert_scratch
        + [dma((weight_copies,)), dma((weight_copies,)), dma((3,))],
        compiler_params=pltpu.CompilerParams(
            collective_id=2, has_side_effects=True, vmem_limit_bytes=VMEM_BYTES
        ),
    )(
        queries,
        keys,
        values,
        lambdas,
        head_gain.reshape(1, -1),
        w_out,
        residual_in,
        norm_gain.reshape(1, -1),
        route_ids,
        route_weight,
        gate,
        up,
        down,
    )


def weight_pieces(weights):
    pieces = [weights]
    for bit in reversed(range(lax.axis_size("tp").bit_length() - 1)):
        pieces = pieces + [
            tuple(swapped(array, "tp", bit) for array in piece) for piece in pieces
        ]
    return pieces


def local(
    queries,
    keys,
    values,
    lambdas,
    head_gain,
    w_out,
    residual_in,
    norm_gain,
    route_ids,
    route_weight,
    w_gate,
    w_up,
    w_down,
):
    sp_size, tp_size = lax.axis_size("sp"), lax.axis_size("tp")
    whole_heads = lambdas.shape[0] * 128 == queries.shape[1]
    square = queries.shape[0] == 2 * 2 * residual_in.shape[0]
    columns_fit = sp_size == 8 and tp_size == 4 and lambdas.shape[0] == 2 and whole_heads and square
    if columns_fit and w_gate.shape[0] == 1:
        tensors = (queries, keys, values, lambdas, head_gain, w_out, residual_in, norm_gain)
        return whole_layer(*tensors, route_ids, route_weight, w_gate[0], w_up[0], w_down[0])
    carried, normed, far_gate, far_up = attend(
        queries,
        keys,
        values,
        lambdas,
        head_gain,
        w_out,
        residual_in,
        norm_gain,
        w_gate.reshape(-1, w_gate.shape[-1]),
        w_up.reshape(-1, w_up.shape[-1]),
    )
    if w_gate.shape[0] == 1 and 4 <= sp_size <= 8 and tp_size == 4:
        named = lax.broadcasted_iota(jnp.int32, (sp_size, residual_in.shape[0], 2), 0)
        shares = jnp.sum(jnp.where(named == route_ids[None], route_weight[None], 0.0), axis=2)
        return expert_layer(
            normed, carried, shares, w_gate[0], w_up[0], w_down[0], far_gate, far_up
        )
    pieces = weight_pieces((w_gate, w_up, w_down))
    carried_wide = carried.astype(jnp.float32)
    dev_rows = residual_in.shape[0]
    model_width = normed.shape[1]
    experts_here = w_gate.shape[0]
    expert_count = experts_here * lax.axis_size("sp")
    capacity = max(2, 4 * dev_rows // expert_count)
    flat_ids = route_ids.reshape(-1)
    targets = flat_ids * capacity + slot_numbers(flat_ids)
    slot_ids = lax.broadcasted_iota(jnp.int32, (expert_count * capacity, dev_rows, 2), 0)
    placement_matrix = jnp.sum(
        (targets.reshape(1, dev_rows, 2) == slot_ids).astype(jnp.int32), axis=2
    ).astype(jnp.bfloat16)
    outgoing = jnp.dot(placement_matrix, normed, preferred_element_type=jnp.float32).astype(
        jnp.bfloat16
    )
    outgoing = outgoing.reshape(lax.axis_size("sp"), experts_here, capacity, model_width)
    arrived = lax.all_to_all(outgoing, "sp", split_axis=0, concat_axis=0, tiled=True)
    summed = 0.0
    for gate_piece, up_piece, down_piece in pieces:
        gate_proj = jnp.einsum("secd,edf->secf", arrived, gate_piece, preferred_element_type=jnp.float32)
        up_proj = jnp.einsum("secd,edf->secf", arrived, up_piece, preferred_element_type=jnp.float32)
        hidden = (jax.nn.silu(gate_proj) * up_proj).astype(jnp.bfloat16)
        summed = summed + jnp.einsum(
            "secf,edf->secd", hidden, down_piece, preferred_element_type=jnp.float32
        )
    returned = send_back(summed.astype(jnp.bfloat16))
    flat_back = returned.reshape(expert_count * capacity, model_width)
    picked = (
        jnp.take(flat_back, targets, axis=0).astype(jnp.float32).reshape(dev_rows, 2, model_width)
    )
    layer_out = carried_wide + jnp.sum(route_weight[..., None] * picked, axis=1)
    return layer_out.astype(jnp.bfloat16)


def solution(mesh):
    placed = (
        P("sp", "tp"),
        P("sp", "tp"),
        P("sp", "tp"),
        P("tp"),
        P(),
        P(),
        P(("sp", "tp"), None),
        P(),
        P(("sp", "tp"), None),
        P(("sp", "tp"), None),
        P("sp", None, "tp"),
        P("sp", None, "tp"),
        P("sp", None, "tp"),
    )
    return jax.shard_map(
        local, mesh=mesh, in_specs=placed, out_specs=P(("sp", "tp"), None), check_vma=False
    )
```
